256 devices in a mesh: sp: 64 (over z, y, core), tp: 4 (over x).
Axes of the slice: x: 4, y: 4, z: 8, core: 2. Of those that a mesh axis runs over, the one named last changes fastest.
Arguments:
- queries: bfloat16 [16384, 2048], P('sp', 'tp'), may hold values from -9 to 9
- keys: bfloat16 [16384, 1024], P('sp', 'tp'), may hold values from -9 to 9
- values: bfloat16 [16384, 1024], P('sp', 'tp'), may hold values from -6 to 6
- lam: float32 [8], P('tp'), may hold values from 0.3 to 0.8
- diff_gain: float32 [256], replicated, may hold values from 0.1 to 1.9
- lin_query: bfloat16 [16384, 512], P('sp', 'tp'), may hold values from -6 to 6
- lin_key: bfloat16 [16384, 512], P('sp', 'tp'), may hold values from -6 to 6
- lin_value: bfloat16 [16384, 1024], P('sp', 'tp'), may hold values from -6 to 6
- decay_pre: float32 [16384, 512], P('sp', 'tp'), may hold values from -14 to 14
- lin_gain: float32 [1024], P('tp'), may hold values from 0.1 to 1.9
- w_out_diff: bfloat16 [2048, 4096], P('tp'), may hold values from -0.125 to 0.125
- w_out_lin: bfloat16 [1024, 4096], P('tp'), may hold values from -0.1875 to 0.1875
Outputs:
- mixed: bfloat16 [16384, 4096], P(('sp', 'tp'))
The draws below stay inside these ranges and needn't reach their ends.
All inputs are finite; a program needn't handle non-finite values.
Results may differ from the reference program's by a relative error of at most 0.015.
Values may be sent and summed in bfloat16 or wider, within the bound.
A program may use at most 128 MiB of HBM per device.

```python
import math
import jax
import jax.numpy as jnp
from jax import lax

D = 4096
DIFF_HEADS = 8
KV_HEADS = 4
LIN_HEADS = 4
HEAD_DIM = 128
KEY_DIM = 128
VAL_DIM = 256
BLOCK = 64
TOK_DEV = 256
SEQUENCE_TOKENS = 16384
N_TP = 4


gate_temp = 16.0


def paired_draw(key):
    query_key = jax.random.fold_in(key, 101)
    key_key = jax.random.fold_in(key, 102)
    query_shape = (SEQUENCE_TOKENS, DIFF_HEADS * 2 * HEAD_DIM)
    key_shape = (SEQUENCE_TOKENS, KV_HEADS * 2 * HEAD_DIM)
    spread = 1.32
    query_rows = jnp.clip(spread * jax.random.normal(query_key, query_shape, jnp.float32), -5.0, 5.0)
    key_rows = jnp.clip(spread * jax.random.normal(key_key, key_shape, jnp.float32), -5.0, 5.0)
    return (query_rows, key_rows)


def draw_queries(key, part):
    return paired_draw(key)[0].astype(jnp.bfloat16)


def draw_keys(key, part):
    return paired_draw(key)[1].astype(jnp.bfloat16)


def draw_decay_pre(key, part):
    width = LIN_HEADS * KEY_DIM
    random_subkeys = jax.random.split(jax.random.fold_in(key, 201), 8)
    fast_share = 0.5
    is_fast = jax.random.uniform(random_subkeys[0], (width,), jnp.float32) < fast_share
    fast_rate = jnp.exp(jax.random.uniform(random_subkeys[1], (width,), jnp.float32, math.log(0.01), math.log(1.0 / 30.0)))
    slow_rate = jnp.exp(jax.random.uniform(random_subkeys[2], (width,), jnp.float32, math.log(0.05), math.log(0.25))) / SEQUENCE_TOKENS
    decay_speed = jnp.where(is_fast, fast_rate, slow_rate)
    processor_factor = jnp.exp(jax.random.uniform(random_subkeys[3], (SEQUENCE_TOKENS // TOK_DEV,), jnp.float32, math.log(0.5), math.log(2.0)))
    processor_factor = jnp.repeat(processor_factor, TOK_DEV)[:, None]
    jaggedness = jax.random.uniform(random_subkeys[4], (SEQUENCE_TOKENS, width), jnp.float32, 0.5, 1.5)
    spike_position = jax.random.randint(random_subkeys[5], (3,), 0, SEQUENCE_TOKENS, dtype=jnp.int32)
    spike_length = jax.random.uniform(random_subkeys[6], (3,), jnp.float32, 0.22, 0.6)
    token_positions = jnp.arange(SEQUENCE_TOKENS, dtype=jnp.int32)
    spike_rows = jnp.sum(jnp.where(token_positions[:, None] == spike_position[None, :], spike_length[None, :], 0.0), axis=1)[:, None]
    logarithm_decay = -(decay_speed[None, :] * processor_factor * jaggedness) - spike_rows
    scaled = gate_temp * logarithm_decay
    return -jnp.log(jnp.expm1(-scaled))


def steps_of(stream_key, dims, cuts, low, high):
    loudness, own = 1.0, jax.random.fold_in(stream_key, 6)
    for position, parts in cuts:
        draws = jnp.exp(jax.random.uniform(jax.random.fold_in(own, position), (parts,), jnp.float32, low / len(cuts), high / len(cuts)))
        loudness = loudness * jnp.repeat(draws, dims[position] // parts).reshape([-1 if axis == position else 1 for axis in range(len(dims))])
    return loudness


def gaussian(stream_key, shape, scale, most, pieces=(), kind=jnp.bfloat16):
    drawn = scale * jax.random.normal(stream_key, shape, jnp.float32)
    if pieces:
        drawn = drawn * steps_of(stream_key, shape, pieces, -0.22, 0.18)
    return jnp.clip(drawn, -most, most).astype(kind)


def setup_inputs(seed: int = 0) -> dict:
    key_of = jax.random.split(jax.random.key(seed), 13)
    queries = draw_queries(jax.random.fold_in(key_of[12], 71), 0)
    keys = draw_keys(jax.random.fold_in(key_of[12], 71), 0)
    values = gaussian(key_of[2], (SEQUENCE_TOKENS, KV_HEADS * VAL_DIM), 1.0, 6.0, ((0, 64), (1, 4)))
    lam = jnp.clip(0.3 + 0.5 * jax.random.uniform(key_of[3], (DIFF_HEADS,), jnp.float32) ** steps_of(key_of[3], (DIFF_HEADS,), ((0, 4),), -0.2, 0.2), 0.3, 0.8)
    diff_gain = jnp.clip(1.0 + 0.18 * jax.random.normal(key_of[4], (VAL_DIM,), jnp.float32), 0.1, 1.9)
    lin_query = gaussian(key_of[5], (SEQUENCE_TOKENS, LIN_HEADS * KEY_DIM), 1.0, 6.0, ((0, 64), (1, 4)))
    lin_key = gaussian(key_of[6], (SEQUENCE_TOKENS, LIN_HEADS * KEY_DIM), 1.0, 6.0, ((0, 64), (1, 4)))
    lin_value = gaussian(key_of[7], (SEQUENCE_TOKENS, LIN_HEADS * VAL_DIM), 1.0, 6.0, ((0, 64), (1, 4)))
    decay_pre = draw_decay_pre(jax.random.fold_in(key_of[12], 71), 0)
    lin_gain = jnp.clip(1.0 + 0.18 * jax.random.normal(key_of[9], (LIN_HEADS * VAL_DIM,), jnp.float32), 0.1, 1.9)
    w_out_diff = gaussian(key_of[10], (DIFF_HEADS * VAL_DIM, D), (DIFF_HEADS * VAL_DIM) ** -0.5, 0.125, ((0, 4),))
    w_out_lin = gaussian(key_of[11], (LIN_HEADS * VAL_DIM, D), (LIN_HEADS * VAL_DIM) ** -0.5, 0.1875, ((0, 4),))
    return {"queries": queries, "keys": keys, "values": values, "lam": lam, "diff_gain": diff_gain, "lin_query": lin_query, "lin_key": lin_key, "lin_value": lin_value, "decay_pre": decay_pre, "lin_gain": lin_gain, "w_out_diff": w_out_diff, "w_out_lin": w_out_lin}


norm_eps = 1e-06
gate_temp = 16.0
neg_large = -1e+30
highest = lax.Precision.HIGHEST

def head_norm(mixed_in, gain):
    return mixed_in * lax.rsqrt(lax.optimization_barrier(jnp.mean(mixed_in * mixed_in, axis=-1, keepdims=True)) + norm_eps) * gain

def one_map(query_rows, key_rows, value_rows, query_pos, key_pos):
    scores = jnp.einsum('jqd,sd->jqs', query_rows, key_rows) / math.sqrt(HEAD_DIM)
    allowed = query_pos[:, None] >= key_pos[None, :]
    scores = jnp.where(allowed, scores, neg_large)
    row_top = lax.optimization_barrier(jnp.max(scores, axis=-1, keepdims=True))
    expo = jnp.where(allowed, jnp.exp(scores - row_top), 0.0)
    totals = lax.optimization_barrier(jnp.sum(expo, axis=-1))
    weights = lax.optimization_barrier(expo.astype(jnp.bfloat16)).astype(jnp.float32)
    numer = jnp.einsum('jqs,se->jqe', weights, value_rows)
    return numer / totals[..., None]

def diff_attention(queries, keys, values, lam, diff_gain):
    group_size = DIFF_HEADS // KV_HEADS
    query_all = queries.astype(jnp.float32).reshape(SEQUENCE_TOKENS, KV_HEADS, group_size, 2, HEAD_DIM)
    key_all = keys.astype(jnp.float32).reshape(SEQUENCE_TOKENS, KV_HEADS, 2, HEAD_DIM)
    value_all = values.astype(jnp.float32).reshape(SEQUENCE_TOKENS, KV_HEADS, VAL_DIM)
    lam_grid = lam.reshape(KV_HEADS, group_size)
    span_rows = math.gcd(SEQUENCE_TOKENS, 1024)
    outputs = []
    for block_index in range(SEQUENCE_TOKENS // span_rows):
        begin = block_index * span_rows
        limit = begin + span_rows
        query_pos = begin + jnp.arange(span_rows, dtype=jnp.int32)
        key_pos = jnp.arange(limit, dtype=jnp.int32)
        query_rows = query_all[begin:limit].transpose(1, 2, 3, 0, 4)
        key_rows = key_all[:limit].transpose(1, 2, 0, 3)
        value_rows = value_all[:limit].transpose(1, 0, 2)

        def per_group(operands):
            query_group, key_group, value_group, lam_group = operands
            first_out = one_map(query_group[:, 0], key_group[0], value_group, query_pos, key_pos)
            second_out = one_map(query_group[:, 1], key_group[1], value_group, query_pos, key_pos)
            return first_out - lam_group[:, None, None] * second_out
        attended = lax.map(per_group, (query_rows, key_rows, value_rows, lam_grid))
        normed = head_norm(attended, diff_gain).astype(jnp.bfloat16)
        outputs.append(normed.transpose(2, 0, 1, 3).reshape(span_rows, DIFF_HEADS * VAL_DIM))
    return jnp.concatenate(outputs, axis=0)

def gla_step(run_state, inputs):
    query_blk, key_blk, value_blk, decay_blk = inputs
    length = query_blk.shape[1]
    cumulative = jnp.cumsum(decay_blk, axis=1)
    lower_mask = jnp.tril(jnp.ones((length, length), dtype=bool))[None, :, :, None]
    spread = jnp.where(lower_mask, cumulative[:, :, None, :] - cumulative[:, None, :, :], 0.0)
    factor = jnp.where(lower_mask, jnp.exp(spread), 0.0)
    inner = jnp.einsum('htd,hsd,htsd->hts', query_blk, key_blk, factor, precision=highest)
    local_part = jnp.einsum('hts,hse->hte', inner, value_blk, precision=highest)
    carried = jnp.einsum('htd,hde->hte', query_blk * jnp.exp(cumulative), run_state, precision=highest)
    last_sum = cumulative[:, -1:, :]
    new_state = jnp.exp(last_sum[:, 0, :])[..., None] * run_state + jnp.einsum('hsd,hse->hde', key_blk * jnp.exp(last_sum - cumulative), value_blk, precision=highest)
    return (new_state, local_part + carried)

def linear_attention(lin_query, lin_key, lin_value, decay_pre, lin_gain):
    block_count = SEQUENCE_TOKENS // BLOCK

    def arrange(array, width):
        return array.astype(jnp.float32).reshape(block_count, BLOCK, LIN_HEADS, width).transpose(0, 2, 1, 3)
    start_state = jnp.zeros((LIN_HEADS, KEY_DIM, VAL_DIM), jnp.float32)
    _, outputs = lax.scan(gla_step, start_state, (arrange(lin_query, KEY_DIM) * KEY_DIM ** (-0.5), arrange(lin_key, KEY_DIM), arrange(lin_value, VAL_DIM), arrange(jax.nn.log_sigmoid(decay_pre) / gate_temp, KEY_DIM)))
    linear_rows = outputs.transpose(0, 2, 1, 3).reshape(SEQUENCE_TOKENS, LIN_HEADS, VAL_DIM)
    normed = head_norm(linear_rows, lin_gain.reshape(LIN_HEADS, VAL_DIM)).astype(jnp.bfloat16)
    return normed.reshape(SEQUENCE_TOKENS, LIN_HEADS * VAL_DIM)

def reference(queries, keys, values, lam, diff_gain, lin_query, lin_key, lin_value, decay_pre, lin_gain, w_out_diff, w_out_lin):
    diff_out = diff_attention(queries, keys, values, lam, diff_gain)
    lin_out = linear_attention(lin_query, lin_key, lin_value, decay_pre, lin_gain)
    diff_cols = DIFF_HEADS * VAL_DIM // N_TP
    lin_cols = LIN_HEADS * VAL_DIM // N_TP
    summed = jnp.zeros((SEQUENCE_TOKENS, D), jnp.float32)
    for member in range(N_TP):
        diff_lo = member * diff_cols
        lin_lo = member * lin_cols
        partial_value = jnp.dot(diff_out[:, diff_lo:diff_lo + diff_cols], w_out_diff[diff_lo:diff_lo + diff_cols], preferred_element_type=jnp.float32)
        partial_value = partial_value + jnp.dot(lin_out[:, lin_lo:lin_lo + lin_cols], w_out_lin[lin_lo:lin_lo + lin_cols], preferred_element_type=jnp.float32)
        partial_value = lax.optimization_barrier(partial_value.astype(jnp.bfloat16)).astype(jnp.float32)
        summed = summed + partial_value
    return summed.astype(jnp.bfloat16)
```

```python
import functools
import math

import jax
import jax.numpy as jnp
from jax import lax
from jax.experimental import pallas as pl
from jax.experimental.pallas import tpu as pltpu
from jax.sharding import Mesh
from jax.sharding import PartitionSpec as P

HEAD_DIM = 128
KEY_DIM = 128
VAL_DIM = 256
BLOCK = 64
SP = ("sp_0", "sp_1", "sp_2")
CHIPS = ("sp_0", "sp_1")
SP_TP = ("sp_0", "sp_1", "sp_2", "tp")

norm_eps = 1e-06
gate_temp = 16.0
neg_large = -1e30
HIGHEST = lax.Precision.HIGHEST
SCORE_SCALE = math.log2(math.e) / math.sqrt(HEAD_DIM)


def head_norm(mixed_in, gain):
    return (
        mixed_in
        * lax.rsqrt(jnp.mean(mixed_in * mixed_in, axis=-1, keepdims=True) + norm_eps)
        * gain
    )


def dot_nt(a, b, precision=None):
    return lax.dot_general(
        a, b, (((1,), (1,)), ((), ())), precision=precision, preferred_element_type=jnp.float32
    )


def dot_tn(a, b, precision=None):
    return lax.dot_general(
        a, b, (((0,), (0,)), ((), ())), precision=precision, preferred_element_type=jnp.float32
    )


def linear_kernel(q_ref, k_ref, v_ref, decay_ref, local_ref, reach_ref, state_ref, total_ref):
    rows = lax.broadcasted_iota(jnp.int32, (BLOCK, BLOCK), 0)
    cols = lax.broadcasted_iota(jnp.int32, (BLOCK, BLOCK), 1)
    lower = rows >= cols
    ones = jnp.where(lower, 1.0, 0.0)
    passed = jnp.zeros((1, KEY_DIM), jnp.float32)
    state = jnp.zeros((KEY_DIM, VAL_DIM), jnp.float32)
    for index in range(q_ref.shape[0] // BLOCK):
        part = slice(index * BLOCK, (index + 1) * BLOCK)
        pre = decay_ref[part, :]
        log_decay = (jnp.minimum(pre, 0.0) - jnp.log1p(jnp.exp(-jnp.abs(pre)))) / gate_temp
        cumulative = jnp.dot(ones, log_decay, precision=HIGHEST, preferred_element_type=jnp.float32)
        query = q_ref[part, :].astype(jnp.float32) * (KEY_DIM**-0.5)
        key = k_ref[part, :].astype(jnp.float32)
        value = v_ref[part, :].astype(jnp.float32)
        query_decayed = query * jnp.exp(cumulative)
        inner = dot_nt(query_decayed, key * jnp.exp(-cumulative), HIGHEST)
        inner = jnp.where(lower, inner, 0.0)
        local = jnp.dot(inner, value, precision=HIGHEST, preferred_element_type=jnp.float32)
        local_ref[part, :] = local + jnp.dot(
            query_decayed, state, precision=HIGHEST, preferred_element_type=jnp.float32
        )
        reach_ref[part, :] = query_decayed * jnp.exp(passed)
        last = cumulative[BLOCK - 1 :, :]
        shrink = jnp.transpose(jnp.broadcast_to(jnp.exp(last), (8, KEY_DIM)))[:, :1]
        state = shrink * state + dot_tn(key * jnp.exp(last - cumulative), value, HIGHEST)
        passed = passed + last
    state_ref[...] = state
    total_ref[...] = jnp.broadcast_to(passed, (8, KEY_DIM))


def absorb(q2_ref, keys, values, top_ref, total_ref, numer_ref, group, hidden):
    scores = dot_nt(q2_ref[group], jnp.concatenate([keys, keys], axis=1))
    if hidden is not None:
        scores = jnp.where(hidden, 2 * neg_large, scores)
    old_top = top_ref[group][:, :1]
    new_top = jnp.maximum(old_top, jnp.max(scores, axis=1, keepdims=True))
    weights = jnp.exp2(scores - new_top)
    shrink = jnp.exp2(old_top - new_top)
    folded = weights[:, :128]
    for tile in range(1, weights.shape[1] // 128):
        folded = folded + weights[:, tile * 128 : (tile + 1) * 128]
    total_ref[group] = total_ref[group] * shrink + folded
    top_ref[group] = jnp.broadcast_to(new_top, (new_top.shape[0], 128))
    numer_ref[group] = numer_ref[group] * shrink + jnp.dot(
        weights.astype(jnp.bfloat16), values, preferred_element_type=jnp.float32
    )


FIRST = 160
SECOND = 96
Z, Y = 8, 4
MESH_IDS = pl.DeviceIdType.MESH
KEY_COLS = slice(0, 2 * HEAD_DIM)
VALUE_COLS = slice(2 * HEAD_DIM, 2 * HEAD_DIM + VAL_DIM)


def remote(src, dst, send, recv, **where):
    return pltpu.make_async_remote_copy(
        src_ref=src,
        dst_ref=dst,
        send_sem=send,
        recv_sem=recv,
        device_id=where,
        device_id_type=MESH_IDS,
    )


def as_column(row):
    return jnp.transpose(jnp.broadcast_to(row, (8, KEY_DIM)))[:, :1]


def mixer_kernel(
    q_hbm,
    k_hbm,
    v_hbm,
    lam_ref,
    diff_gain_ref,
    lin_q_ref,
    lin_k_ref,
    lin_v_ref,
    decay_ref,
    lin_gain_ref,
    act_ref,
    kva,
    kvb,
    both_q,
    q2_ref,
    top_ref,
    total_ref,
    numer_ref,
    stat_ref,
    far_stat,
    far_numer,
    local_ref,
    reach_ref,
    core_state,
    core_decay,
    chip_state,
    chip_decay,
    chain_ref,
    own_sems,
    recv_a,
    recv_b,
    send_az,
    send_ay,
    send_af,
    send_by,
    send_bf,
    send_bz,
    pair_send,
    pair_recv,
    line_send,
    line_recv,
    chain_send,
    chain_recv,
):
    z, y, core = (lax.axis_index(name) for name in SP)
    tok_rows = q_hbm.shape[0]
    chip_rows = 2 * tok_rows
    up, down = lax.rem(z + 1, Z), lax.rem(z + Z - 1, Z)
    east, west = lax.rem(y + 1, Y), lax.rem(y + Y - 1, Y)
    across = lax.rem(y + 2, Y)
    other = 1 - core

    owned = [
        pltpu.make_async_copy(
            k_hbm.at[pl.ds(0, FIRST)], kva.at[z, y, :, KEY_COLS], own_sems.at[0]
        ),
        pltpu.make_async_copy(
            v_hbm.at[pl.ds(0, FIRST)], kva.at[z, y, :, VALUE_COLS], own_sems.at[1]
        ),
        pltpu.make_async_copy(
            k_hbm.at[pl.ds(FIRST, SECOND)], kvb.at[z, y, :, KEY_COLS], own_sems.at[2]
        ),
        pltpu.make_async_copy(
            v_hbm.at[pl.ds(FIRST, SECOND)], kvb.at[z, y, :, VALUE_COLS], own_sems.at[3]
        ),
        pltpu.make_async_copy(q_hbm, both_q.at[core], own_sems.at[4]),
    ]
    for copy in owned:
        copy.start()
    barrier = pltpu.get_barrier_semaphore()
    for where in (
        {"sp_0": up},
        {"sp_0": down},
        {"sp_1": east},
        {"sp_1": west},
        {"sp_1": across},
        {"sp_2": other},
    ):
        pl.semaphore_signal(barrier, inc=1, device_id=where, device_id_type=MESH_IDS)
    pl.semaphore_wait(barrier, 6)
    for copy in owned:
        copy.wait()

    def a_z(zo, toward, way, cols=slice(None), half=0):
        block = kva.at[zo, y, :, cols]
        return remote(block, block, send_az.at[zo, way], recv_a.at[zo, y, half], sp_0=toward)

    def a_y(zo, toward, way):
        block = kva.at[zo, y]
        return remote(block, block, send_ay.at[zo, way], recv_a.at[zo, y, 0], sp_1=toward)

    def a_far(zo, yo, toward, way):
        block = kva.at[zo, yo, :, (KEY_COLS, VALUE_COLS)[way]]
        return remote(block, block, send_af.at[zo, way], recv_a.at[zo, yo, way], sp_1=toward)

    def a_wait(zo, yo, cols=slice(None), half=0):
        block = kva.at[zo, yo, :, cols]
        remote(block, block, send_az.at[zo, 0], recv_a.at[zo, yo, half], sp_0=up).wait_recv()

    def b_y(toward, way):
        block = kvb.at[z, y]
        return remote(block, block, send_by.at[way], recv_b.at[z, y, 0], sp_1=toward)

    def b_far(yo, toward, way):
        block = kvb.at[z, yo, :, (KEY_COLS, VALUE_COLS)[way]]
        return remote(block, block, send_bf.at[way], recv_b.at[z, yo, way], sp_1=toward)

    def b_z(zo, yo, toward, way, cols=slice(None), half=0):
        block = kvb.at[zo, yo, :, cols]
        return remote(block, block, send_bz.at[zo, yo, way], recv_b.at[zo, yo, half], sp_0=toward)

    def b_wait(zo, yo, cols=slice(None), half=0):
        block = kvb.at[zo, yo, :, cols]
        remote(block, block, send_bz.at[zo, yo, 0], recv_b.at[zo, yo, half], sp_0=up).wait_recv()

    pair_q = remote(
        both_q.at[core], both_q.at[core], pair_send.at[0], pair_recv.at[0], sp_2=other
    )
    pair_q.start()
    a_z(z, up, 0).start()
    a_z(z, down, 1).start()
    b_y(east, 0).start()
    b_y(west, 1).start()
    a_y(z, east, 0).start()
    a_y(z, west, 1).start()
    b_z(z, y, up, 0).start()
    b_z(z, y, down, 1).start()

    linear_kernel(
        lin_q_ref,
        lin_k_ref,
        lin_v_ref,
        decay_ref,
        local_ref,
        reach_ref,
        core_state.at[core],
        core_decay.at[core],
    )
    pair_state = remote(
        core_state.at[core], core_state.at[core], pair_send.at[1], pair_recv.at[1], sp_2=other
    )
    pair_decay = remote(
        core_decay.at[core], core_decay.at[core], pair_send.at[2], pair_recv.at[2], sp_2=other
    )
    pair_state.start()
    pair_decay.start()

    b_wait(z, west)
    b_far(west, east, 0).start()
    b_z(z, west, up, 0).start()
    b_z(z, west, down, 1).start()
    b_wait(z, east)
    b_far(east, west, 1).start()
    b_z(z, east, up, 0).start()
    b_z(z, east, down, 1).start()

    top_ref[...] = jnp.full_like(top_ref, neg_large)
    total_ref[...] = jnp.zeros_like(total_ref)
    numer_ref[...] = jnp.zeros_like(numer_ref)
    pair_q.wait_recv()
    for group in range(4):
        mapping, head = group // 2, group % 2
        first = (head * 2 + mapping) * HEAD_DIM
        for side in range(2):
            scaled = both_q[side, :, first : first + HEAD_DIM].astype(jnp.float32) * SCORE_SCALE
            high = scaled.astype(jnp.bfloat16)
            low = (scaled - high.astype(jnp.float32)).astype(jnp.bfloat16)
            part = slice(side * tok_rows, (side + 1) * tok_rows)
            q2_ref[group, part, :HEAD_DIM] = high
            q2_ref[group, part, HEAD_DIM:] = low

    pair_state.wait_recv()
    pair_decay.wait_recv()
    chip_state[y] = (
        as_column(jnp.exp(core_decay[1][:1])) * core_state[0] + core_state[1]
    ).astype(jnp.bfloat16)
    chip_decay[y] = core_decay[0] + core_decay[1]

    b_wait(z, across, KEY_COLS, 0)
    b_wait(z, across, VALUE_COLS, 1)
    b_z(z, across, up, 0).start()
    b_z(z, across, down, 1).start()

    def line(peer, index):
        return (
            remote(
                chip_state.at[y],
                chip_state.at[y],
                line_send.at[index, 0],
                line_recv.at[y, 0],
                sp_1=peer,
            ),
            remote(
                chip_decay.at[y],
                chip_decay.at[y],
                line_send.at[index, 1],
                line_recv.at[y, 1],
                sp_1=peer,
            ),
        )

    for index, peer in enumerate((east, west, across)):
        for copy in line(peer, index):
            copy.start()

    def chain_copy():
        return remote(
            chain_ref.at[1], chain_ref.at[0], chain_send.at[0], chain_recv.at[0], sp_0=up
        )

    def follow(state, yo):
        return as_column(jnp.exp(chip_decay[yo][:1])) * state + chip_state[yo].astype(jnp.float32)

    def pass_on():
        state = chain_ref[0]
        for yo in range(Y):
            state = follow(state, yo)
        chain_ref[1] = state
        chain_copy().start()

    @pl.when(z == 0)
    def _():
        chain_ref[0] = jnp.zeros_like(chain_ref[0])

    order = lambda index: lax.rem(
        y + jnp.where(index == 0, 0, jnp.where(index == 1, Y - 1, jnp.where(index == 2, 1, 2))), Y
    )
    origin = lambda unit: lax.rem(
        z + 2 * Z + jnp.where(lax.rem(unit, 2) == 1, -((unit + 1) // 2), unit // 2), Z
    )

    def compute(store, zo, group, hidden):
        mapping = group // 2
        tokens = store.shape[2]
        first = pl.multiple_of(mapping * HEAD_DIM, HEAD_DIM)
        keys = store[zo, :, :, pl.ds(first, HEAD_DIM)].reshape(Y * tokens, HEAD_DIM)
        values = store[zo, :, :, VALUE_COLS].reshape(Y * tokens, VAL_DIM)
        absorb(q2_ref, keys, values, top_ref, total_ref, numer_ref, group, hidden)

    def hidden_from(tokens, start):
        column = lax.broadcasted_iota(jnp.int32, (chip_rows, Y * tokens), 1)
        row = lax.broadcasted_iota(jnp.int32, (chip_rows, Y * tokens), 0)
        chip = jnp.zeros_like(column)
        for index in range(1, Y):
            chip = chip + jnp.where(column >= index * tokens, 1, 0)
        key_pos = column + chip * (chip_rows - tokens) + core * tok_rows + start
        return key_pos > y * chip_rows + row

    def a_step(distance):
        for way, zo, toward in (
            (0, lax.rem(z + Z - distance, Z), up),
            (1, lax.rem(z + distance, Z), down),
        ):
            a_wait(zo, y)

            @pl.when(distance < 3)
            def _():
                a_z(zo, toward, way).start()

            @pl.when(distance == 3)
            def _():
                a_z(zo, toward, way, (KEY_COLS, VALUE_COLS)[way], way).start()

            a_y(zo, east, 0).start()
            a_y(zo, west, 1).start()

    def a_near(zo):
        a_wait(zo, west)
        a_far(zo, west, east, 0).start()
        a_wait(zo, east)
        a_far(zo, east, west, 1).start()

    def half_step(h, carry):
        @pl.when(h <= 2)
        def _():
            a_step(h + 1)

        @pl.when(h == 3)
        def _():
            zo = lax.rem(z + 4, Z)
            a_wait(zo, y, KEY_COLS, 0)
            a_wait(zo, y, VALUE_COLS, 1)
            a_y(zo, east, 0).start()
            a_y(zo, west, 1).start()

        @pl.when(h == 0)
        def _():
            a_near(z)

        @pl.when((h == 2) | (h == 4) | (h == 6))
        def _():
            a_near(lax.rem(z + Z - h // 2, Z))
            a_near(lax.rem(z + h // 2, Z))

        @pl.when(h == 8)
        def _():
            a_near(lax.rem(z + 4, Z))

        a_unit, b_unit = h - 2, h - 1
        a_origin, b_origin = origin(jnp.maximum(a_unit, 0)), origin(jnp.maximum(b_unit, 0))

        @pl.when(h >= 2)
        def _():
            a_wait(a_origin, across, KEY_COLS, 0)
            a_wait(a_origin, across, VALUE_COLS, 1)

        def piece(j, inner):
            distance = h // 2 + 1
            yo = order(lax.rem(h, 2) * 2 + j // 2)
            ahead, behind = lax.rem(z + Z - distance, Z), lax.rem(z + distance, Z)

            @pl.when((h <= 5) & (lax.rem(j, 2) == 0))
            def _():
                b_wait(ahead, yo)

                @pl.when(distance < 3)
                def _():
                    b_z(ahead, yo, up, 0).start()

                @pl.when(distance == 3)
                def _():
                    b_z(ahead, yo, up, 0, KEY_COLS, 0).start()

            @pl.when((h <= 5) & (lax.rem(j, 2) == 1))
            def _():
                b_wait(behind, yo)

                @pl.when(distance < 3)
                def _():
                    b_z(behind, yo, down, 1).start()

                @pl.when(distance == 3)
                def _():
                    b_z(behind, yo, down, 1, VALUE_COLS, 1).start()

            @pl.when(((h == 6) | (h == 7)) & (lax.rem(j, 2) == 1))
            def _():
                b_wait(ahead, yo, KEY_COLS, 0)
                b_wait(ahead, yo, VALUE_COLS, 1)

            slot = (h - 1) * 2 + j // 2

            @pl.when((h >= 1) & (lax.rem(j, 2) == 0) & (slot == z))
            def _():
                @pl.when(z > 0)
                def _():
                    chain_copy().wait_recv()

                @pl.when(z < Z - 1)
                def _():
                    pass_on()

            @pl.when((h >= 2) & (a_unit > 0) & (a_origin < z))
            def _():
                compute(kva, a_origin, j, None)

            @pl.when(a_unit == 0)
            def _():
                compute(kva, z, j, hidden_from(FIRST, 0))

            @pl.when((b_unit > 0) & (h <= 8) & (b_origin < z))
            def _():
                compute(kvb, b_origin, j, None)

            @pl.when(b_unit == 0)
            def _():
                compute(kvb, z, j, hidden_from(SECOND, FIRST))

            return inner

        @pl.when(h == 1)
        def _():
            for peer in (east, west, across):
                for part, buffer in enumerate((chip_state, chip_decay)):
                    remote(
                        buffer.at[peer],
                        buffer.at[peer],
                        line_send.at[0, part],
                        line_recv.at[peer, part],
                        sp_1=peer,
                    ).wait_recv()

        return lax.fori_loop(0, 4, piece, carry)

    lax.fori_loop(0, 10, half_step, 0)

    lane = lax.broadcasted_iota(jnp.int32, (chip_rows, 128), 1)
    for group in range(4):
        summed = jnp.sum(total_ref[group], axis=1, keepdims=True)
        stat_ref[group] = jnp.where(lane < 64, top_ref[group], summed)
    theirs = pl.ds(pl.multiple_of(other * tok_rows, tok_rows), tok_rows)
    mine = pl.ds(pl.multiple_of(core * tok_rows, tok_rows), tok_rows)
    swap_numer = remote(
        numer_ref.at[:, theirs], far_numer, pair_send.at[3], pair_recv.at[3], sp_2=other
    )
    swap_stat = remote(
        stat_ref.at[:, theirs], far_stat, pair_send.at[4], pair_recv.at[4], sp_2=other
    )
    swap_numer.start()
    swap_stat.start()

    state = chain_ref[0]
    for yo in range(Y - 1):
        state = jnp.where(yo < y, follow(state, yo), state)
    after = as_column(jnp.exp(core_decay[0][:1])) * state + core_state[0]
    state = jnp.where(core == 1, after, state)
    rows = local_ref[...] + jnp.dot(
        reach_ref[...], state, precision=HIGHEST, preferred_element_type=jnp.float32
    )
    act_ref[:, 2 * VAL_DIM :] = head_norm(rows, lin_gain_ref[...]).astype(act_ref.dtype)

    swap_numer.wait_recv()
    swap_stat.wait_recv()

    def merged(group):
        near, far = stat_ref[group, mine], far_stat[group]
        near_top, far_top = near[:, :1], far[:, :1]
        both_top = jnp.maximum(near_top, far_top)
        near_scale, far_scale = jnp.exp2(near_top - both_top), jnp.exp2(far_top - both_top)
        total = near[:, 64:65] * near_scale + far[:, 64:65] * far_scale
        numer = numer_ref[group, mine] * near_scale + far_numer[group] * far_scale
        return numer / total

    for head in range(2):
        attended = merged(head) - lam_ref[head] * merged(2 + head)
        act_ref[:, head * VAL_DIM : (head + 1) * VAL_DIM] = head_norm(
            attended, diff_gain_ref[...]
        ).astype(act_ref.dtype)

    for copy in (pair_q, pair_state, pair_decay, swap_numer, swap_stat):
        copy.wait_send()
    for index, peer in enumerate((east, west, across)):
        for copy in line(peer, index):
            copy.wait_send()

    @pl.when(z < Z - 1)
    def _():
        chain_copy().wait_send()

    for way, toward in ((0, east), (1, west)):
        b_y(toward, way).wait_send()
        b_far(west if way == 0 else east, toward, way).wait_send()

    def drain(offset, carry):
        zo = lax.rem(z + offset, Z)
        for way, toward in ((0, east), (1, west)):
            a_y(zo, toward, way).wait_send()
            a_far(zo, west if way == 0 else east, toward, way).wait_send()
        return carry

    lax.fori_loop(0, Z, drain, 0)
    for way, toward, sign, cols in ((0, up, -1, KEY_COLS), (1, down, 1, VALUE_COLS)):

        def drain_z(distance, carry):
            zo = lax.rem(z + Z + sign * distance, Z)
            a_z(zo, toward, way).wait_send()
            for yo in range(Y):
                b_z(zo, yo, toward, way).wait_send()
            return carry

        lax.fori_loop(0, 3, drain_z, 0)
        zo = lax.rem(z + Z + sign * 3, Z)
        a_z(zo, toward, way, cols, way).wait_send()
        for yo in range(Y):
            b_z(zo, yo, toward, way, cols, way).wait_send()


def mixer(
    queries, keys, values, lam, diff_gain, lin_query, lin_key, lin_value, decay_pre, lin_gain
):
    tok_rows = queries.shape[0]
    rows = 2 * tok_rows
    width = 2 * HEAD_DIM + VAL_DIM
    in_hbm = pl.BlockSpec(memory_space=pl.ANY)
    in_vmem = pl.BlockSpec(memory_space=pltpu.VMEM)
    dma = pltpu.SemaphoreType.DMA
    return pl.pallas_call(
        mixer_kernel,
        out_shape=jax.ShapeDtypeStruct((tok_rows, 3 * VAL_DIM), jnp.bfloat16),
        in_specs=[in_hbm] * 3 + [pl.BlockSpec(memory_space=pltpu.SMEM)] + [in_vmem] * 6,
        out_specs=in_vmem,
        scratch_shapes=[
            pltpu.VMEM((Z, Y, FIRST, width), jnp.bfloat16),
            pltpu.VMEM((Z, Y, SECOND, width), jnp.bfloat16),
            pltpu.VMEM((2, tok_rows, 4 * HEAD_DIM), jnp.bfloat16),
            pltpu.VMEM((4, rows, 2 * HEAD_DIM), jnp.bfloat16),
            pltpu.VMEM((4, rows, 128), jnp.float32),
            pltpu.VMEM((4, rows, 128), jnp.float32),
            pltpu.VMEM((4, rows, VAL_DIM), jnp.float32),
            pltpu.VMEM((4, rows, 128), jnp.float32),
            pltpu.VMEM((4, tok_rows, 128), jnp.float32),
            pltpu.VMEM((4, tok_rows, VAL_DIM), jnp.float32),
            pltpu.VMEM((tok_rows, VAL_DIM), jnp.float32),
            pltpu.VMEM((tok_rows, KEY_DIM), jnp.float32),
            pltpu.VMEM((2, KEY_DIM, VAL_DIM), jnp.float32),
            pltpu.VMEM((2, 8, KEY_DIM), jnp.float32),
            pltpu.VMEM((Y, KEY_DIM, VAL_DIM), jnp.bfloat16),
            pltpu.VMEM((Y, 8, KEY_DIM), jnp.float32),
            pltpu.VMEM((2, KEY_DIM, VAL_DIM), jnp.float32),
            dma((5,)),
            dma((Z, Y, 2)),
            dma((Z, Y, 2)),
            dma((Z, 2)),
            dma((Z, 2)),
            dma((Z, 2)),
            dma((2,)),
            dma((2,)),
            dma((Z, Y, 2)),
            dma((5,)),
            dma((5,)),
            dma((3, 2)),
            dma((Y, 2)),
            dma((1,)),
            dma((1,)),
        ],
        compiler_params=pltpu.CompilerParams(
            collective_id=0, has_side_effects=True, vmem_limit_bytes=60 * 1024 * 1024
        ),
        cost_estimate=pl.CostEstimate(
            flops=12 * 10**9, bytes_accessed=16 * 10**6, transcendentals=16 * 10**6
        ),
    )(
        queries,
        keys,
        values,
        lam,
        diff_gain.reshape(1, VAL_DIM),
        lin_query,
        lin_key,
        lin_value,
        decay_pre,
        lin_gain.reshape(1, VAL_DIM),
    )


def body(
    queries,
    keys,
    values,
    lam,
    diff_gain,
    lin_query,
    lin_key,
    lin_value,
    decay_pre,
    lin_gain,
    w_out_diff,
    w_out_lin,
):
    tok_rows = queries.shape[0]
    act = mixer(
        queries, keys, values, lam, diff_gain, lin_query, lin_key, lin_value, decay_pre, lin_gain
    )
    mixed = (
        jnp.dot(act[:, : 2 * VAL_DIM], w_out_diff, preferred_element_type=jnp.float32)
        + jnp.dot(act[:, 2 * VAL_DIM :], w_out_lin, preferred_element_type=jnp.float32)
    ).astype(jnp.bfloat16)
    blocks = mixed.reshape(4, tok_rows // 4, -1)
    arrived = lax.all_to_all(blocks, "tp", split_axis=0, concat_axis=0, tiled=True)
    return arrived.astype(jnp.float32).sum(axis=0).astype(jnp.bfloat16)


def solution(mesh):
    finer = Mesh(mesh.devices.reshape(8, 4, 2, mesh.shape["tp"]), ("sp_0", "sp_1", "sp_2", "tp"))
    in_specs = (
        P(SP, "tp"),
        P(SP, "tp"),
        P(SP, "tp"),
        P("tp"),
        P(),
        P(SP, "tp"),
        P(SP, "tp"),
        P(SP, "tp"),
        P(SP, "tp"),
        P("tp"),
        P("tp", None),
        P("tp", None),
    )
    out_specs = P(SP_TP, None)
    return jax.shard_map(body, mesh=finer, in_specs=in_specs, out_specs=out_specs, check_vma=False)
```

```python
import functools
import math

import jax
import jax.numpy as jnp
from jax import lax
from jax.experimental import pallas as pl
from jax.experimental.pallas import tpu as pltpu
from jax.sharding import Mesh
from jax.sharding import PartitionSpec as P

HEAD_DIM = 128
KEY_DIM = 128
VAL_DIM = 256
BLOCK = 64
SP = ("sp_0", "sp_1", "sp_2")
CHIPS = ("sp_0", "sp_1")
SP_TP = ("sp_0", "sp_1", "sp_2", "tp")

norm_eps = 1e-06
gate_temp = 16.0
neg_large = -1e30
HIGHEST = lax.Precision.HIGHEST
SCORE_SCALE = math.log2(math.e) / math.sqrt(HEAD_DIM)


def head_norm(mixed_in, gain):
    return (
        mixed_in
        * lax.rsqrt(jnp.mean(mixed_in * mixed_in, axis=-1, keepdims=True) + norm_eps)
        * gain
    )


def dot_nt(a, b, precision=None):
    return lax.dot_general(
        a, b, (((1,), (1,)), ((), ())), precision=precision, preferred_element_type=jnp.float32
    )


def dot_tn(a, b, precision=None):
    return lax.dot_general(
        a, b, (((0,), (0,)), ((), ())), precision=precision, preferred_element_type=jnp.float32
    )


def linear_kernel(q_ref, k_ref, v_ref, decay_ref, local_ref, reach_ref, state_ref, total_ref):
    rows = lax.broadcasted_iota(jnp.int32, (BLOCK, BLOCK), 0)
    cols = lax.broadcasted_iota(jnp.int32, (BLOCK, BLOCK), 1)
    lower = rows >= cols
    ones = jnp.where(lower, 1.0, 0.0)
    passed = jnp.zeros((1, KEY_DIM), jnp.float32)
    state = jnp.zeros((KEY_DIM, VAL_DIM), jnp.float32)
    for index in range(q_ref.shape[0] // BLOCK):
        part = slice(index * BLOCK, (index + 1) * BLOCK)
        pre = decay_ref[part, :]
        log_decay = (jnp.minimum(pre, 0.0) - jnp.log1p(jnp.exp(-jnp.abs(pre)))) / gate_temp
        cumulative = jnp.dot(ones, log_decay, precision=HIGHEST, preferred_element_type=jnp.float32)
        query = q_ref[part, :].astype(jnp.float32) * (KEY_DIM**-0.5)
        key = k_ref[part, :].astype(jnp.float32)
        value = v_ref[part, :].astype(jnp.float32)
        query_decayed = query * jnp.exp(cumulative)
        inner = dot_nt(query_decayed, key * jnp.exp(-cumulative), HIGHEST)
        inner = jnp.where(lower, inner, 0.0)
        local = jnp.dot(inner, value, precision=HIGHEST, preferred_element_type=jnp.float32)
        local_ref[part, :] = local + jnp.dot(
            query_decayed, state, precision=HIGHEST, preferred_element_type=jnp.float32
        )
        reach_ref[part, :] = query_decayed * jnp.exp(passed)
        last = cumulative[BLOCK - 1 :, :]
        shrink = jnp.transpose(jnp.broadcast_to(jnp.exp(last), (8, KEY_DIM)))[:, :1]
        state = shrink * state + dot_tn(key * jnp.exp(last - cumulative), value, HIGHEST)
        passed = passed + last
    state_ref[...] = state
    total_ref[...] = jnp.broadcast_to(passed, (8, KEY_DIM))


def absorb(q2_ref, keys, values, top_ref, total_ref, numer_ref, hidden):
    scores = dot_nt(q2_ref[...], jnp.concatenate([keys, keys], axis=1))
    if hidden is not None:
        scores = jnp.where(hidden, 2 * neg_large, scores)
    old_top = top_ref[:, :1]
    new_top = jnp.maximum(old_top, jnp.max(scores, axis=1, keepdims=True))
    weights = jnp.exp2(scores - new_top)
    shrink = jnp.exp2(old_top - new_top)
    folded = weights[:, :128]
    for tile in range(1, weights.shape[1] // 128):
        folded = folded + weights[:, tile * 128 : (tile + 1) * 128]
    total_ref[...] = total_ref[...] * shrink + folded
    top_ref[...] = jnp.broadcast_to(new_top, top_ref.shape)
    numer_ref[...] = numer_ref[...] * shrink + jnp.dot(
        weights.astype(jnp.bfloat16), values, preferred_element_type=jnp.float32
    )


PER_PIECE = 4
CHUNK = 256
FIRST = 160
SECOND = 96
Z, Y, TP = 8, 4, 4
COLUMNS = 1024
MESH_IDS = pl.DeviceIdType.MESH
KEY_COLS = slice(0, 2 * HEAD_DIM)
VALUE_COLS = slice(2 * HEAD_DIM, 2 * HEAD_DIM + VAL_DIM)


def remote(src, dst, send, recv, **where):
    return pltpu.make_async_remote_copy(
        src_ref=src,
        dst_ref=dst,
        send_sem=send,
        recv_sem=recv,
        device_id=where,
        device_id_type=MESH_IDS,
    )


def as_column(row):
    return jnp.transpose(jnp.broadcast_to(row, (8, KEY_DIM)))[:, :1]


def mixer_kernel(
    q_hbm,
    k_hbm,
    v_hbm,
    lam_ref,
    diff_gain_ref,
    lin_q_ref,
    lin_k_ref,
    lin_v_ref,
    decay_ref,
    lin_gain_ref,
    w_diff_hbm,
    w_lin_hbm,
    out_ref,
    act_ref,
    w_ref,
    part_ref,
    far_in,
    near_out,
    near_in,
    kva,
    kvb,
    both_q,
    q2_ref,
    top_ref,
    total_ref,
    numer_ref,
    stat_ref,
    far_stat,
    far_numer,
    local_ref,
    reach_ref,
    core_state,
    core_decay,
    chip_state,
    chip_decay,
    chain_ref,
    own_sems,
    recv_a,
    recv_b,
    send_az,
    send_ay,
    send_af,
    send_by,
    send_bf,
    send_bz,
    pair_send,
    pair_recv,
    line_send,
    line_recv,
    chain_send,
    chain_recv,
    weight_sems,
    far_send,
    far_recv,
    near_send,
    near_recv,
):
    z, y, core = (lax.axis_index(name) for name in SP)
    tok_rows = q_hbm.shape[0]
    chip_rows = 2 * tok_rows
    up, down = lax.rem(z + 1, Z), lax.rem(z + Z - 1, Z)
    east, west = lax.rem(y + 1, Y), lax.rem(y + Y - 1, Y)
    across = lax.rem(y + 2, Y)
    other = 1 - core
    x = lax.axis_index("tp")
    right, left = lax.rem(x + 1, TP), lax.rem(x + TP - 1, TP)

    owned = [
        pltpu.make_async_copy(
            k_hbm.at[pl.ds(0, FIRST)], kva.at[z, y, :, KEY_COLS], own_sems.at[0]
        ),
        pltpu.make_async_copy(
            v_hbm.at[pl.ds(0, FIRST)], kva.at[z, y, :, VALUE_COLS], own_sems.at[1]
        ),
        pltpu.make_async_copy(
            k_hbm.at[pl.ds(FIRST, SECOND)], kvb.at[z, y, :, KEY_COLS], own_sems.at[2]
        ),
        pltpu.make_async_copy(
            v_hbm.at[pl.ds(FIRST, SECOND)], kvb.at[z, y, :, VALUE_COLS], own_sems.at[3]
        ),
        pltpu.make_async_copy(q_hbm, both_q.at[core], own_sems.at[4]),
    ]
    for copy in owned:
        copy.start()
    barrier = pltpu.get_barrier_semaphore()
    for where in (
        {"sp_0": up},
        {"sp_0": down},
        {"sp_1": east},
        {"sp_1": west},
        {"sp_1": across},
        {"sp_2": other},
        {"tp": right},
        {"tp": left},
    ):
        pl.semaphore_signal(barrier, inc=1, device_id=where, device_id_type=MESH_IDS)
    pl.semaphore_wait(barrier, 8)
    for copy in owned:
        copy.wait()

    def a_z(zo, toward, way, cols=slice(None), half=0):
        block = kva.at[zo, y, :, cols]
        return remote(block, block, send_az.at[zo, way], recv_a.at[zo, y, half], sp_0=toward)

    def a_y(zo, toward, way):
        block = kva.at[zo, y]
        return remote(block, block, send_ay.at[zo, way], recv_a.at[zo, y, 0], sp_1=toward)

    def a_far(zo, yo, toward, way):
        block = kva.at[zo, yo, :, (KEY_COLS, VALUE_COLS)[way]]
        return remote(block, block, send_af.at[zo, way], recv_a.at[zo, yo, way], sp_1=toward)

    def a_wait(zo, yo, cols=slice(None), half=0):
        block = kva.at[zo, yo, :, cols]
        remote(block, block, send_az.at[zo, 0], recv_a.at[zo, yo, half], sp_0=up).wait_recv()

    def b_y(toward, way):
        block = kvb.at[z, y]
        return remote(block, block, send_by.at[way], recv_b.at[z, y, 0], sp_1=toward)

    def b_far(yo, toward, way):
        block = kvb.at[z, yo, :, (KEY_COLS, VALUE_COLS)[way]]
        return remote(block, block, send_bf.at[way], recv_b.at[z, yo, way], sp_1=toward)

    def b_z(zo, yo, toward, way, cols=slice(None), half=0):
        block = kvb.at[zo, yo, :, cols]
        return remote(block, block, send_bz.at[zo, yo, way], recv_b.at[zo, yo, half], sp_0=toward)

    def b_wait(zo, yo, cols=slice(None), half=0):
        block = kvb.at[zo, yo, :, cols]
        remote(block, block, send_bz.at[zo, yo, 0], recv_b.at[zo, yo, half], sp_0=up).wait_recv()

    pair_q = remote(
        both_q.at[core], both_q.at[core], pair_send.at[0], pair_recv.at[0], sp_2=other
    )
    pair_q.start()
    def outward(copy_of):
        @pl.when(z < Z - 1)
        def _():
            copy_of(up, 0).start()

        @pl.when(z < Z // 2)
        def _():
            copy_of(down, 1).start()

    outward(lambda toward, way: a_z(z, toward, way))
    b_y(east, 0).start()
    b_y(west, 1).start()
    a_y(z, east, 0).start()
    a_y(z, west, 1).start()
    outward(lambda toward, way: b_z(z, y, toward, way))

    linear_kernel(
        lin_q_ref,
        lin_k_ref,
        lin_v_ref,
        decay_ref,
        local_ref,
        reach_ref,
        core_state.at[core],
        core_decay.at[core],
    )
    pair_state = remote(
        core_state.at[core], core_state.at[core], pair_send.at[1], pair_recv.at[1], sp_2=other
    )
    pair_decay = remote(
        core_decay.at[core], core_decay.at[core], pair_send.at[2], pair_recv.at[2], sp_2=other
    )
    pair_state.start()
    pair_decay.start()

    b_wait(z, west)
    b_far(west, east, 0).start()
    outward(lambda toward, way: b_z(z, west, toward, way))
    b_wait(z, east)
    b_far(east, west, 1).start()
    outward(lambda toward, way: b_z(z, east, toward, way))

    weights = (
        pltpu.make_async_copy(w_diff_hbm, w_ref.at[pl.ds(0, 2 * VAL_DIM)], weight_sems.at[0]),
        pltpu.make_async_copy(
            w_lin_hbm, w_ref.at[pl.ds(2 * VAL_DIM, VAL_DIM)], weight_sems.at[1]
        ),
    )
    for copy in weights:
        copy.start()

    top_ref[...] = jnp.full_like(top_ref, neg_large)
    total_ref[...] = jnp.zeros_like(total_ref)
    numer_ref[...] = jnp.zeros_like(numer_ref)
    pair_q.wait_recv()
    for group in range(4):
        mapping, head = group // 2, group % 2
        first = (head * 2 + mapping) * HEAD_DIM
        for side in range(2):
            scaled = both_q[side, :, first : first + HEAD_DIM].astype(jnp.float32) * SCORE_SCALE
            high = scaled.astype(jnp.bfloat16)
            low = (scaled - high.astype(jnp.float32)).astype(jnp.bfloat16)
            part = slice(side * tok_rows, (side + 1) * tok_rows)
            q2_ref[group, part, :HEAD_DIM] = high
            q2_ref[group, part, HEAD_DIM:] = low

    pair_state.wait_recv()
    pair_decay.wait_recv()
    chip_state[y] = (
        as_column(jnp.exp(core_decay[1][:1])) * core_state[0] + core_state[1]
    ).astype(jnp.bfloat16)
    chip_decay[y] = core_decay[0] + core_decay[1]

    b_wait(z, across, KEY_COLS, 0)
    b_wait(z, across, VALUE_COLS, 1)
    outward(lambda toward, way: b_z(z, across, toward, way))

    def line(peer, index):
        return (
            remote(
                chip_state.at[y],
                chip_state.at[y],
                line_send.at[index, 0],
                line_recv.at[y, 0],
                sp_1=peer,
            ),
            remote(
                chip_decay.at[y],
                chip_decay.at[y],
                line_send.at[index, 1],
                line_recv.at[y, 1],
                sp_1=peer,
            ),
        )

    for index, peer in enumerate((east, west, across)):
        for copy in line(peer, index):
            copy.start()

    def chain_copy():
        return remote(
            chain_ref.at[1], chain_ref.at[0], chain_send.at[0], chain_recv.at[0], sp_0=up
        )

    def follow(state, yo):
        return as_column(jnp.exp(chip_decay[yo][:1])) * state + chip_state[yo].astype(jnp.float32)

    def pass_on():
        state = chain_ref[0]
        for yo in range(Y):
            state = follow(state, yo)
        chain_ref[1] = state
        chain_copy().start()

    @pl.when(z == 0)
    def _():
        chain_ref[0] = jnp.zeros_like(chain_ref[0])

    order = lambda index: lax.rem(
        y + jnp.where(index == 0, 0, jnp.where(index == 1, Y - 1, jnp.where(index == 2, 1, 2))), Y
    )
    origin = lambda unit: lax.rem(
        z + 2 * Z + jnp.where(lax.rem(unit, 2) == 1, -((unit + 1) // 2), unit // 2), Z
    )

    def compute(zo, index, hidden):
        values = jnp.concatenate(
            [
                store[zo, :, :, VALUE_COLS].reshape(Y * store.shape[2], VAL_DIM)
                for store in (kva, kvb)
            ],
            axis=0,
        )
        for step in range(PER_PIECE):
            group = index * PER_PIECE + step
            first = pl.multiple_of(group // 2 * HEAD_DIM, HEAD_DIM)
            keys = jnp.concatenate(
                [
                    store[zo, :, :, pl.ds(first, HEAD_DIM)].reshape(
                        Y * store.shape[2], HEAD_DIM
                    )
                    for store in (kva, kvb)
                ],
                axis=0,
            )
            for part in range(0, chip_rows, CHUNK):
                rows = slice(part, part + CHUNK)
                absorb(
                    q2_ref.at[group, rows],
                    keys,
                    values,
                    top_ref.at[group, rows],
                    total_ref.at[group, rows],
                    numer_ref.at[group, rows],
                    None if hidden is None else hidden[rows],
                )

    def hidden_keys():
        column = lax.broadcasted_iota(jnp.int32, (chip_rows, Y * tok_rows), 1)
        row = lax.broadcasted_iota(jnp.int32, (chip_rows, Y * tok_rows), 0)
        key_pos = column + core * tok_rows
        for index in range(1, Y):
            key_pos = key_pos + jnp.where(column >= index * FIRST, chip_rows - FIRST, 0)
        key_pos = key_pos + jnp.where(
            column >= Y * FIRST, FIRST - Y * FIRST - (Y - 1) * (chip_rows - FIRST), 0
        )
        for index in range(1, Y):
            key_pos = key_pos + jnp.where(
                column >= Y * FIRST + index * SECOND, chip_rows - SECOND, 0
            )
        return key_pos > y * chip_rows + row

    def a_step(distance):
        ahead, behind = lax.rem(z + Z - distance, Z), lax.rem(z + distance, Z)

        @pl.when(z >= distance)
        def _():
            a_wait(ahead, y)

            @pl.when((distance < 3) & (z < Z - 1))
            def _():
                a_z(ahead, up, 0).start()

            @pl.when((distance == 3) & (z < Z - 1))
            def _():
                a_z(ahead, up, 0, KEY_COLS, 0).start()

            a_y(ahead, east, 0).start()
            a_y(ahead, west, 1).start()

        @pl.when(behind < Z // 2)
        def _():
            a_wait(behind, y)

            @pl.when(distance < 3)
            def _():
                a_z(behind, down, 1).start()

            @pl.when(distance == 3)
            def _():
                a_z(behind, down, 1, VALUE_COLS, 1).start()

            @pl.when(behind < z)
            def _():
                a_y(behind, east, 0).start()
                a_y(behind, west, 1).start()

    def a_near(zo):
        @pl.when(zo <= z)
        def _():
            a_wait(zo, west)
            a_far(zo, west, east, 0).start()
            a_wait(zo, east)
            a_far(zo, east, west, 1).start()

    def half_step(h, carry):
        @pl.when(h <= 2)
        def _():
            a_step(h + 1)

        @pl.when((h == 3) & (z >= Z // 2))
        def _():
            zo = lax.rem(z + 4, Z)
            a_wait(zo, y, KEY_COLS, 0)
            a_wait(zo, y, VALUE_COLS, 1)
            a_y(zo, east, 0).start()
            a_y(zo, west, 1).start()

        @pl.when(h == 0)
        def _():
            a_near(z)

        @pl.when((h == 2) | (h == 4) | (h == 6))
        def _():
            a_near(lax.rem(z + Z - h // 2, Z))
            a_near(lax.rem(z + h // 2, Z))

        @pl.when(h == 8)
        def _():
            a_near(lax.rem(z + 4, Z))

        unit = h - 2
        zo_unit = origin(jnp.maximum(unit, 0))

        @pl.when((unit == 0) | ((unit > 0) & (zo_unit < z)))
        def _():
            a_wait(zo_unit, across, KEY_COLS, 0)
            a_wait(zo_unit, across, VALUE_COLS, 1)

        def event(j):
            distance = h // 2 + 1
            yo = order(lax.rem(h, 2) * 2 + j // 2)
            ahead, behind = lax.rem(z + Z - distance, Z), lax.rem(z + distance, Z)

            @pl.when((h <= 5) & (lax.rem(j, 2) == 0) & (z >= distance))
            def _():
                b_wait(ahead, yo)

                @pl.when((distance < 3) & (z < Z - 1))
                def _():
                    b_z(ahead, yo, up, 0).start()

                @pl.when((distance == 3) & (z < Z - 1))
                def _():
                    b_z(ahead, yo, up, 0, KEY_COLS, 0).start()

            @pl.when((h <= 5) & (lax.rem(j, 2) == 1) & (behind < Z // 2))
            def _():
                b_wait(behind, yo)

                @pl.when(distance < 3)
                def _():
                    b_z(behind, yo, down, 1).start()

                @pl.when(distance == 3)
                def _():
                    b_z(behind, yo, down, 1, VALUE_COLS, 1).start()

            @pl.when(((h == 6) | (h == 7)) & (lax.rem(j, 2) == 1) & (z >= Z // 2))
            def _():
                b_wait(ahead, yo, KEY_COLS, 0)
                b_wait(ahead, yo, VALUE_COLS, 1)

            slot = (h - 1) * 2 + j // 2

            @pl.when((h >= 1) & (lax.rem(j, 2) == 0) & (slot == z))
            def _():
                @pl.when(z > 0)
                def _():
                    chain_copy().wait_recv()

                @pl.when(z < Z - 1)
                def _():
                    pass_on()

        def piece(j, inner):
            for step in range(PER_PIECE):
                event(j * PER_PIECE + step)

            @pl.when((unit > 0) & (zo_unit < z))
            def _():
                compute(zo_unit, j, None)

            @pl.when(unit == 0)
            def _():
                compute(z, j, hidden_keys())

            return inner

        @pl.when(h == 1)
        def _():
            for peer in (east, west, across):
                for part, buffer in enumerate((chip_state, chip_decay)):
                    remote(
                        buffer.at[peer],
                        buffer.at[peer],
                        line_send.at[0, part],
                        line_recv.at[peer, part],
                        sp_1=peer,
                    ).wait_recv()

        return lax.fori_loop(0, 4 // PER_PIECE, piece, carry)

    lax.fori_loop(0, 10, half_step, 0)

    lane = lax.broadcasted_iota(jnp.int32, (chip_rows, 128), 1)
    for group in range(4):
        summed = jnp.sum(total_ref[group], axis=1, keepdims=True)
        stat_ref[group] = jnp.where(lane < 64, top_ref[group], summed)
    theirs = pl.ds(pl.multiple_of(other * tok_rows, tok_rows), tok_rows)
    mine = pl.ds(pl.multiple_of(core * tok_rows, tok_rows), tok_rows)
    swap_numer = remote(
        numer_ref.at[:, theirs], far_numer, pair_send.at[3], pair_recv.at[3], sp_2=other
    )
    swap_stat = remote(
        stat_ref.at[:, theirs], far_stat, pair_send.at[4], pair_recv.at[4], sp_2=other
    )
    swap_numer.start()
    swap_stat.start()

    state = chain_ref[0]
    for yo in range(Y - 1):
        state = jnp.where(yo < y, follow(state, yo), state)
    after = as_column(jnp.exp(core_decay[0][:1])) * state + core_state[0]
    state = jnp.where(core == 1, after, state)
    rows = local_ref[...] + jnp.dot(
        reach_ref[...], state, precision=HIGHEST, preferred_element_type=jnp.float32
    )
    act_ref[:, 2 * VAL_DIM :] = head_norm(rows, lin_gain_ref[...]).astype(act_ref.dtype)

    swap_numer.wait_recv()
    swap_stat.wait_recv()

    def merged(group):
        near, far = stat_ref[group, mine], far_stat[group]
        near_top, far_top = near[:, :1], far[:, :1]
        both_top = jnp.maximum(near_top, far_top)
        near_scale, far_scale = jnp.exp2(near_top - both_top), jnp.exp2(far_top - both_top)
        total = near[:, 64:65] * near_scale + far[:, 64:65] * far_scale
        numer = numer_ref[group, mine] * near_scale + far_numer[group] * far_scale
        return numer / total

    for head in range(2):
        attended = merged(head) - lam_ref[head] * merged(2 + head)
        act_ref[:, head * VAL_DIM : (head + 1) * VAL_DIM] = head_norm(
            attended, diff_gain_ref[...]
        ).astype(act_ref.dtype)

    own_rows = tok_rows // TP
    half = COLUMNS // 2
    halves = (slice(0, half), slice(half, COLUMNS))
    rows_of = lambda member: pl.ds(pl.multiple_of(member * own_rows, own_rows), own_rows)
    toward = (right, left)
    opposite = lax.rem(x + 2, TP)
    for copy in weights:
        copy.wait()

    def far_copy(chunk, way):
        return remote(
            part_ref.at[chunk, rows_of(opposite), halves[way]],
            far_in.at[chunk, way],
            far_send.at[chunk, way],
            far_recv.at[chunk, way],
            tp=toward[way],
        )

    def near_copy(chunk, way):
        return remote(
            near_out.at[chunk, way],
            near_in.at[chunk, way],
            near_send.at[chunk, way],
            near_recv.at[chunk, way],
            tp=toward[way],
        )

    chunks = part_ref.shape[0]

    def project(chunk, carry):
        first = pl.multiple_of(chunk * COLUMNS, COLUMNS)
        part_ref[chunk] = jnp.dot(
            act_ref[...], w_ref[:, pl.ds(first, COLUMNS)], preferred_element_type=jnp.float32
        ).astype(part_ref.dtype)
        for way in range(2):
            far_copy(chunk, way).start()
        return carry

    lax.fori_loop(0, chunks, project, 0)

    def meet(chunk, carry):
        for way in range(2):
            far_copy(chunk, way).wait_recv()
            near = part_ref[chunk, rows_of(toward[way])].astype(jnp.float32)
            here = near[:, halves[way]] + far_in[chunk, way].astype(jnp.float32)
            sides = (here, near[:, halves[1]]) if way == 0 else (near[:, halves[0]], here)
            near_out[chunk, way] = jnp.concatenate(sides, axis=1).astype(near_out.dtype)
            near_copy(chunk, way).start()
        return carry

    lax.fori_loop(0, chunks, meet, 0)

    def finish(chunk, carry):
        total = part_ref[chunk, rows_of(x)].astype(jnp.float32)
        for way in range(2):
            near_copy(chunk, way).wait_recv()
            total = total + near_in[chunk, way].astype(jnp.float32)
        first = pl.multiple_of(chunk * COLUMNS, COLUMNS)
        out_ref[:, pl.ds(first, COLUMNS)] = total.astype(out_ref.dtype)
        return carry

    lax.fori_loop(0, chunks, finish, 0)

    def drain_out(chunk, carry):
        for way in range(2):
            far_copy(chunk, way).wait_send()
            near_copy(chunk, way).wait_send()
        return carry

    lax.fori_loop(0, chunks, drain_out, 0)
    for copy in (pair_q, pair_state, pair_decay, swap_numer, swap_stat):
        copy.wait_send()
    for index, peer in enumerate((east, west, across)):
        for copy in line(peer, index):
            copy.wait_send()

    @pl.when(z < Z - 1)
    def _():
        chain_copy().wait_send()

    for way, toward in ((0, east), (1, west)):
        b_y(toward, way).wait_send()
        b_far(west if way == 0 else east, toward, way).wait_send()

    def drain(offset, carry):
        zo = z - offset
        for way, toward in ((0, east), (1, west)):
            a_y(zo, toward, way).wait_send()
            a_far(zo, west if way == 0 else east, toward, way).wait_send()
        return carry

    lax.fori_loop(0, z + 1, drain, 0)

    @pl.when(z < Z - 1)
    def _():
        def drain_up(offset, carry):
            a_z(z - offset, up, 0).wait_send()
            for yo in range(Y):
                b_z(z - offset, yo, up, 0).wait_send()
            return carry

        lax.fori_loop(0, jnp.minimum(z + 1, 3), drain_up, 0)

        @pl.when(z >= 3)
        def _():
            a_z(z - 3, up, 0, KEY_COLS, 0).wait_send()
            for yo in range(Y):
                b_z(z - 3, yo, up, 0, KEY_COLS, 0).wait_send()

    for distance in range(4):
        zo = lax.rem(z + distance, Z)
        part = (VALUE_COLS, 1) if distance == 3 else ()

        @pl.when(zo < Z // 2)
        def _(zo=zo, part=part):
            a_z(zo, down, 1, *part).wait_send()
            for yo in range(Y):
                b_z(zo, yo, down, 1, *part).wait_send()


def body(
    queries,
    keys,
    values,
    lam,
    diff_gain,
    lin_query,
    lin_key,
    lin_value,
    decay_pre,
    lin_gain,
    w_out_diff,
    w_out_lin,
):
    tok_rows = queries.shape[0]
    depth = w_out_diff.shape[0] + w_out_lin.shape[0]
    model = w_out_diff.shape[1]
    chunks, own_rows = model // COLUMNS, tok_rows // TP
    rows = 2 * tok_rows
    width = 2 * HEAD_DIM + VAL_DIM
    in_hbm = pl.BlockSpec(memory_space=pl.ANY)
    in_vmem = pl.BlockSpec(memory_space=pltpu.VMEM)
    dma = pltpu.SemaphoreType.DMA
    return pl.pallas_call(
        mixer_kernel,
        out_shape=jax.ShapeDtypeStruct((own_rows, model), jnp.bfloat16),
        in_specs=[in_hbm] * 3
        + [pl.BlockSpec(memory_space=pltpu.SMEM)]
        + [in_vmem] * 6
        + [in_hbm] * 2,
        out_specs=in_vmem,
        scratch_shapes=[
            pltpu.VMEM((tok_rows, 3 * VAL_DIM), jnp.bfloat16),
            pltpu.VMEM((depth, model), jnp.bfloat16),
            pltpu.VMEM((chunks, tok_rows, COLUMNS), jnp.bfloat16),
            pltpu.VMEM((chunks, 2, own_rows, COLUMNS // 2), jnp.bfloat16),
            pltpu.VMEM((chunks, 2, own_rows, COLUMNS), jnp.bfloat16),
            pltpu.VMEM((chunks, 2, own_rows, COLUMNS), jnp.bfloat16),
            pltpu.VMEM((Z, Y, FIRST, width), jnp.bfloat16),
            pltpu.VMEM((Z, Y, SECOND, width), jnp.bfloat16),
            pltpu.VMEM((2, tok_rows, 4 * HEAD_DIM), jnp.bfloat16),
            pltpu.VMEM((4, rows, 2 * HEAD_DIM), jnp.bfloat16),
            pltpu.VMEM((4, rows, 128), jnp.float32),
            pltpu.VMEM((4, rows, 128), jnp.float32),
            pltpu.VMEM((4, rows, VAL_DIM), jnp.float32),
            pltpu.VMEM((4, rows, 128), jnp.float32),
            pltpu.VMEM((4, tok_rows, 128), jnp.float32),
            pltpu.VMEM((4, tok_rows, VAL_DIM), jnp.float32),
            pltpu.VMEM((tok_rows, VAL_DIM), jnp.float32),
            pltpu.VMEM((tok_rows, KEY_DIM), jnp.float32),
            pltpu.VMEM((2, KEY_DIM, VAL_DIM), jnp.float32),
            pltpu.VMEM((2, 8, KEY_DIM), jnp.float32),
            pltpu.VMEM((Y, KEY_DIM, VAL_DIM), jnp.bfloat16),
            pltpu.VMEM((Y, 8, KEY_DIM), jnp.float32),
            pltpu.VMEM((2, KEY_DIM, VAL_DIM), jnp.float32),
            dma((5,)),
            dma((Z, Y, 2)),
            dma((Z, Y, 2)),
            dma((Z, 2)),
            dma((Z, 2)),
            dma((Z, 2)),
            dma((2,)),
            dma((2,)),
            dma((Z, Y, 2)),
            dma((5,)),
            dma((5,)),
            dma((3, 2)),
            dma((Y, 2)),
            dma((1,)),
            dma((1,)),
            dma((2,)),
            dma((chunks, 2)),
            dma((chunks, 2)),
            dma((chunks, 2)),
            dma((chunks, 2)),
        ],
        compiler_params=pltpu.CompilerParams(
            collective_id=0, has_side_effects=True, vmem_limit_bytes=60 * 1024 * 1024
        ),
        cost_estimate=pl.CostEstimate(
            flops=12 * 10**9, bytes_accessed=16 * 10**6, transcendentals=16 * 10**6
        ),
    )(
        queries,
        keys,
        values,
        lam,
        diff_gain.reshape(1, VAL_DIM),
        lin_query,
        lin_key,
        lin_value,
        decay_pre,
        lin_gain.reshape(1, VAL_DIM),
        w_out_diff,
        w_out_lin,
    )


def solution(mesh):
    finer = Mesh(mesh.devices.reshape(8, 4, 2, mesh.shape["tp"]), ("sp_0", "sp_1", "sp_2", "tp"))
    in_specs = (
        P(SP, "tp"),
        P(SP, "tp"),
        P(SP, "tp"),
        P("tp"),
        P(),
        P(SP, "tp"),
        P(SP, "tp"),
        P(SP, "tp"),
        P(SP, "tp"),
        P("tp"),
        P("tp", None),
        P("tp", None),
    )
    out_specs = P(SP_TP, None)
    return jax.shard_map(body, mesh=finer, in_specs=in_specs, out_specs=out_specs, check_vma=False)
```

```python
import functools
import math

import jax
import jax.numpy as jnp
from jax import lax
from jax.experimental import pallas as pl
from jax.experimental.pallas import tpu as pltpu
from jax.sharding import Mesh
from jax.sharding import PartitionSpec as P

HEAD_DIM = 128
KEY_DIM = 128
VAL_DIM = 256
BLOCK = 64
SP = ("sp_0", "sp_1", "sp_2")
CHIPS = ("sp_0", "sp_1")
SP_TP = ("sp_0", "sp_1", "sp_2", "tp")

norm_eps = 1e-06
gate_temp = 16.0
neg_large = -1e30
HIGHEST = lax.Precision.HIGHEST
SCORE_SCALE = math.log2(math.e) / math.sqrt(HEAD_DIM)


def head_norm(mixed_in, gain):
    return (
        mixed_in
        * lax.rsqrt(jnp.mean(mixed_in * mixed_in, axis=-1, keepdims=True) + norm_eps)
        * gain
    )


def dot_nt(a, b, precision=None):
    return lax.dot_general(
        a, b, (((1,), (1,)), ((), ())), precision=precision, preferred_element_type=jnp.float32
    )


def dot_tn(a, b, precision=None):
    return lax.dot_general(
        a, b, (((0,), (0,)), ((), ())), precision=precision, preferred_element_type=jnp.float32
    )


def linear_kernel(q_ref, k_ref, v_ref, decay_ref, local_ref, reach_ref, state_ref, total_ref):
    rows = lax.broadcasted_iota(jnp.int32, (BLOCK, BLOCK), 0)
    cols = lax.broadcasted_iota(jnp.int32, (BLOCK, BLOCK), 1)
    lower = rows >= cols
    ones = jnp.where(lower, 1.0, 0.0)
    passed = jnp.zeros((1, KEY_DIM), jnp.float32)
    state = jnp.zeros((KEY_DIM, VAL_DIM), jnp.float32)
    for index in range(q_ref.shape[0] // BLOCK):
        part = slice(index * BLOCK, (index + 1) * BLOCK)
        pre = decay_ref[part, :]
        log_decay = (jnp.minimum(pre, 0.0) - jnp.log1p(jnp.exp(-jnp.abs(pre)))) / gate_temp
        cumulative = jnp.dot(ones, log_decay, precision=HIGHEST, preferred_element_type=jnp.float32)
        query = q_ref[part, :].astype(jnp.float32) * (KEY_DIM**-0.5)
        key = k_ref[part, :].astype(jnp.float32)
        value = v_ref[part, :].astype(jnp.float32)
        query_decayed = query * jnp.exp(cumulative)
        inner = dot_nt(query_decayed, key * jnp.exp(-cumulative), HIGHEST)
        inner = jnp.where(lower, inner, 0.0)
        local = jnp.dot(inner, value, precision=HIGHEST, preferred_element_type=jnp.float32)
        local_ref[part, :] = local + jnp.dot(
            query_decayed, state, precision=HIGHEST, preferred_element_type=jnp.float32
        )
        reach_ref[part, :] = query_decayed * jnp.exp(passed)
        last = cumulative[BLOCK - 1 :, :]
        shrink = jnp.transpose(jnp.broadcast_to(jnp.exp(last), (8, KEY_DIM)))[:, :1]
        state = shrink * state + dot_tn(key * jnp.exp(last - cumulative), value, HIGHEST)
        passed = passed + last
    state_ref[...] = state
    total_ref[...] = jnp.broadcast_to(passed, (8, KEY_DIM))


def absorb(q2_ref, keys, values, top_ref, total_ref, numer_ref, hidden):
    scores = dot_nt(q2_ref[...], jnp.concatenate([keys, keys], axis=1))
    if hidden is not None:
        scores = jnp.where(hidden, 2 * neg_large, scores)
    old_top = top_ref[:, :1]
    new_top = jnp.maximum(old_top, jnp.max(scores, axis=1, keepdims=True))
    weights = jnp.exp2(scores - new_top)
    shrink = jnp.exp2(old_top - new_top)
    folded = weights[:, :128]
    for tile in range(1, weights.shape[1] // 128):
        folded = folded + weights[:, tile * 128 : (tile + 1) * 128]
    total_ref[...] = total_ref[...] * shrink + folded
    top_ref[...] = jnp.broadcast_to(new_top, top_ref.shape)
    numer_ref[...] = numer_ref[...] * shrink + jnp.dot(
        weights.astype(jnp.bfloat16), values, preferred_element_type=jnp.float32
    )


PER_PIECE = 4
CHUNK = 256
FIRST = 160
SECOND = 96
Z, Y, TP = 8, 4, 4
COLUMNS = 1024
MESH_IDS = pl.DeviceIdType.MESH
KEY_COLS = slice(0, 2 * HEAD_DIM)
VALUE_COLS = slice(2 * HEAD_DIM, 2 * HEAD_DIM + VAL_DIM)


def remote(src, dst, send, recv, **where):
    return pltpu.make_async_remote_copy(
        src_ref=src,
        dst_ref=dst,
        send_sem=send,
        recv_sem=recv,
        device_id=where,
        device_id_type=MESH_IDS,
    )


def as_column(row):
    return jnp.transpose(jnp.broadcast_to(row, (8, KEY_DIM)))[:, :1]


def mixer_kernel(
    q_hbm,
    k_hbm,
    v_hbm,
    lam_ref,
    diff_gain_ref,
    lin_q_ref,
    lin_k_ref,
    lin_v_ref,
    decay_ref,
    lin_gain_ref,
    w_diff_hbm,
    w_lin_hbm,
    out_ref,
    act_ref,
    w_ref,
    part_ref,
    far_in,
    near_out,
    near_in,
    kva,
    kvb,
    both_q,
    q2_ref,
    top_ref,
    total_ref,
    numer_ref,
    stat_ref,
    far_stat,
    far_numer,
    local_ref,
    reach_ref,
    core_state,
    core_decay,
    chip_state,
    chip_decay,
    chain_ref,
    own_sems,
    recv_a,
    recv_b,
    send_az,
    send_ay,
    send_af,
    send_by,
    send_bf,
    send_bz,
    pair_send,
    pair_recv,
    line_send,
    line_recv,
    chain_send,
    chain_recv,
    weight_sems,
    far_send,
    far_recv,
    near_send,
    near_recv,
):
    z, y, core = (lax.axis_index(name) for name in SP)
    tok_rows = q_hbm.shape[0]
    chip_rows = 2 * tok_rows
    up, down = lax.rem(z + 1, Z), lax.rem(z + Z - 1, Z)
    east, west = lax.rem(y + 1, Y), lax.rem(y + Y - 1, Y)
    across = lax.rem(y + 2, Y)
    other = 1 - core
    x = lax.axis_index("tp")
    right, left = lax.rem(x + 1, TP), lax.rem(x + TP - 1, TP)

    owned = [
        pltpu.make_async_copy(
            k_hbm.at[pl.ds(0, FIRST)], kva.at[z, y, :, KEY_COLS], own_sems.at[0]
        ),
        pltpu.make_async_copy(
            v_hbm.at[pl.ds(0, FIRST)], kva.at[z, y, :, VALUE_COLS], own_sems.at[1]
        ),
        pltpu.make_async_copy(
            k_hbm.at[pl.ds(FIRST, SECOND)], kvb.at[z, y, :, KEY_COLS], own_sems.at[2]
        ),
        pltpu.make_async_copy(
            v_hbm.at[pl.ds(FIRST, SECOND)], kvb.at[z, y, :, VALUE_COLS], own_sems.at[3]
        ),
        pltpu.make_async_copy(q_hbm, both_q.at[core], own_sems.at[4]),
    ]
    for copy in owned:
        copy.start()
    barrier = pltpu.get_barrier_semaphore()
    for where in (
        {"sp_0": up},
        {"sp_0": down},
        {"sp_1": east},
        {"sp_1": west},
        {"sp_1": across},
        {"sp_2": other},
        {"tp": right},
        {"tp": left},
    ):
        pl.semaphore_signal(barrier, inc=1, device_id=where, device_id_type=MESH_IDS)
    pl.semaphore_wait(barrier, 8)
    for copy in owned:
        copy.wait()

    def a_z(zo, toward, way, cols=slice(None), half=0):
        block = kva.at[zo, y, :, cols]
        return remote(block, block, send_az.at[zo, way], recv_a.at[zo, y, half], sp_0=toward)

    def a_y(zo, toward, way):
        block = kva.at[zo, y]
        return remote(block, block, send_ay.at[zo, way], recv_a.at[zo, y, 0], sp_1=toward)

    def a_far(zo, yo, toward, way):
        block = kva.at[zo, yo, :, (KEY_COLS, VALUE_COLS)[way]]
        return remote(block, block, send_af.at[zo, way], recv_a.at[zo, yo, way], sp_1=toward)

    def a_wait(zo, yo, cols=slice(None), half=0):
        block = kva.at[zo, yo, :, cols]
        remote(block, block, send_az.at[zo, 0], recv_a.at[zo, yo, half], sp_0=up).wait_recv()

    def b_y(toward, way):
        block = kvb.at[z, y]
        return remote(block, block, send_by.at[way], recv_b.at[z, y, 0], sp_1=toward)

    def b_far(yo, toward, way):
        block = kvb.at[z, yo, :, (KEY_COLS, VALUE_COLS)[way]]
        return remote(block, block, send_bf.at[way], recv_b.at[z, yo, way], sp_1=toward)

    def b_z(zo, yo, toward, way, cols=slice(None), half=0):
        block = kvb.at[zo, yo, :, cols]
        return remote(block, block, send_bz.at[zo, yo, way], recv_b.at[zo, yo, half], sp_0=toward)

    def b_wait(zo, yo, cols=slice(None), half=0):
        block = kvb.at[zo, yo, :, cols]
        remote(block, block, send_bz.at[zo, yo, 0], recv_b.at[zo, yo, half], sp_0=up).wait_recv()

    pair_q = remote(
        both_q.at[core], both_q.at[core], pair_send.at[0], pair_recv.at[0], sp_2=other
    )
    pair_q.start()
    def outward(copy_of):
        @pl.when(z < Z - 1)
        def _():
            copy_of(up, 0).start()

        @pl.when(z < Z // 2)
        def _():
            copy_of(down, 1).start()

    outward(lambda toward, way: a_z(z, toward, way))
    b_y(east, 0).start()
    b_y(west, 1).start()
    a_y(z, east, 0).start()
    a_y(z, west, 1).start()
    outward(lambda toward, way: b_z(z, y, toward, way))

    linear_kernel(
        lin_q_ref,
        lin_k_ref,
        lin_v_ref,
        decay_ref,
        local_ref,
        reach_ref,
        core_state.at[core],
        core_decay.at[core],
    )
    pair_state = remote(
        core_state.at[core], core_state.at[core], pair_send.at[1], pair_recv.at[1], sp_2=other
    )
    pair_decay = remote(
        core_decay.at[core], core_decay.at[core], pair_send.at[2], pair_recv.at[2], sp_2=other
    )
    pair_state.start()
    pair_decay.start()

    def a_step(distance):
        ahead, behind = lax.rem(z + Z - distance, Z), lax.rem(z + distance, Z)

        @pl.when(z >= distance)
        def _():
            a_wait(ahead, y)

            @pl.when((distance < 3) & (z < Z - 1))
            def _():
                a_z(ahead, up, 0).start()

            @pl.when((distance == 3) & (z < Z - 1))
            def _():
                a_z(ahead, up, 0, KEY_COLS, 0).start()

            a_y(ahead, east, 0).start()
            a_y(ahead, west, 1).start()

        @pl.when(behind < Z // 2)
        def _():
            a_wait(behind, y)

            @pl.when(distance < 3)
            def _():
                a_z(behind, down, 1).start()

            @pl.when(distance == 3)
            def _():
                a_z(behind, down, 1, VALUE_COLS, 1).start()

            @pl.when(behind < z)
            def _():
                a_y(behind, east, 0).start()
                a_y(behind, west, 1).start()

    a_step(jnp.int32(1))

    b_wait(z, west)
    b_far(west, east, 0).start()
    outward(lambda toward, way: b_z(z, west, toward, way))
    b_wait(z, east)
    b_far(east, west, 1).start()
    outward(lambda toward, way: b_z(z, east, toward, way))

    weights = (
        pltpu.make_async_copy(w_diff_hbm, w_ref.at[pl.ds(0, 2 * VAL_DIM)], weight_sems.at[0]),
        pltpu.make_async_copy(
            w_lin_hbm, w_ref.at[pl.ds(2 * VAL_DIM, VAL_DIM)], weight_sems.at[1]
        ),
    )
    for copy in weights:
        copy.start()

    top_ref[...] = jnp.full_like(top_ref, neg_large)
    total_ref[...] = jnp.zeros_like(total_ref)
    numer_ref[...] = jnp.zeros_like(numer_ref)
    pair_q.wait_recv()
    for group in range(4):
        mapping, head = group // 2, group % 2
        first = (head * 2 + mapping) * HEAD_DIM
        for side in range(2):
            scaled = both_q[side, :, first : first + HEAD_DIM].astype(jnp.float32) * SCORE_SCALE
            high = scaled.astype(jnp.bfloat16)
            low = (scaled - high.astype(jnp.float32)).astype(jnp.bfloat16)
            part = slice(side * tok_rows, (side + 1) * tok_rows)
            q2_ref[group, part, :HEAD_DIM] = high
            q2_ref[group, part, HEAD_DIM:] = low

    pair_state.wait_recv()
    pair_decay.wait_recv()
    chip_state[y] = (
        as_column(jnp.exp(core_decay[1][:1])) * core_state[0] + core_state[1]
    ).astype(jnp.bfloat16)
    chip_decay[y] = core_decay[0] + core_decay[1]

    b_wait(z, across, KEY_COLS, 0)
    b_wait(z, across, VALUE_COLS, 1)
    outward(lambda toward, way: b_z(z, across, toward, way))

    def line(peer, index):
        return (
            remote(
                chip_state.at[y],
                chip_state.at[y],
                line_send.at[index, 0],
                line_recv.at[y, 0],
                sp_1=peer,
            ),
            remote(
                chip_decay.at[y],
                chip_decay.at[y],
                line_send.at[index, 1],
                line_recv.at[y, 1],
                sp_1=peer,
            ),
        )

    for index, peer in enumerate((east, west, across)):
        for copy in line(peer, index):
            copy.start()

    def chain_copy():
        return remote(
            chain_ref.at[1], chain_ref.at[0], chain_send.at[0], chain_recv.at[0], sp_0=up
        )

    def follow(state, yo):
        return as_column(jnp.exp(chip_decay[yo][:1])) * state + chip_state[yo].astype(jnp.float32)

    def pass_on():
        state = chain_ref[0]
        for yo in range(Y):
            state = follow(state, yo)
        chain_ref[1] = state
        chain_copy().start()

    @pl.when(z == 0)
    def _():
        chain_ref[0] = jnp.zeros_like(chain_ref[0])

    order = lambda index: lax.rem(
        y + jnp.where(index == 0, 0, jnp.where(index == 1, Y - 1, jnp.where(index == 2, 1, 2))), Y
    )
    origin = lambda unit: lax.rem(
        z + 2 * Z + jnp.where(lax.rem(unit, 2) == 1, -((unit + 1) // 2), unit // 2), Z
    )

    def compute(zo, index, hidden):
        values = jnp.concatenate(
            [
                store[zo, :, :, VALUE_COLS].reshape(Y * store.shape[2], VAL_DIM)
                for store in (kva, kvb)
            ],
            axis=0,
        )
        for step in range(PER_PIECE):
            group = index * PER_PIECE + step
            first = pl.multiple_of(group // 2 * HEAD_DIM, HEAD_DIM)
            keys = jnp.concatenate(
                [
                    store[zo, :, :, pl.ds(first, HEAD_DIM)].reshape(
                        Y * store.shape[2], HEAD_DIM
                    )
                    for store in (kva, kvb)
                ],
                axis=0,
            )
            for part in range(0, chip_rows, CHUNK):
                rows = slice(part, part + CHUNK)
                absorb(
                    q2_ref.at[group, rows],
                    keys,
                    values,
                    top_ref.at[group, rows],
                    total_ref.at[group, rows],
                    numer_ref.at[group, rows],
                    None if hidden is None else hidden[rows],
                )

    def hidden_keys():
        column = lax.broadcasted_iota(jnp.int32, (chip_rows, Y * tok_rows), 1)
        row = lax.broadcasted_iota(jnp.int32, (chip_rows, Y * tok_rows), 0)
        key_pos = column + core * tok_rows
        for index in range(1, Y):
            key_pos = key_pos + jnp.where(column >= index * FIRST, chip_rows - FIRST, 0)
        key_pos = key_pos + jnp.where(
            column >= Y * FIRST, FIRST - Y * FIRST - (Y - 1) * (chip_rows - FIRST), 0
        )
        for index in range(1, Y):
            key_pos = key_pos + jnp.where(
                column >= Y * FIRST + index * SECOND, chip_rows - SECOND, 0
            )
        return key_pos > y * chip_rows + row

    def a_near(zo):
        @pl.when(zo <= z)
        def _():
            a_wait(zo, west)
            a_far(zo, west, east, 0).start()
            a_wait(zo, east)
            a_far(zo, east, west, 1).start()

    def half_step(h, carry):
        @pl.when((h == 0) | (h == 2))
        def _():
            a_step(2 + h // 2)

        @pl.when((h == 3) & (z >= Z // 2))
        def _():
            zo = lax.rem(z + 4, Z)
            a_wait(zo, y, KEY_COLS, 0)
            a_wait(zo, y, VALUE_COLS, 1)
            a_y(zo, east, 0).start()
            a_y(zo, west, 1).start()

        @pl.when(h == 0)
        def _():
            a_near(z)

        @pl.when((h == 3) | (h == 5))
        def _():
            a_near(lax.rem(z + Z - (h + 1) // 2, Z))
            a_near(lax.rem(z + (h + 1) // 2, Z))

        @pl.when(h == 6)
        def _():
            a_near(lax.rem(z + 4, Z))

        unit = h - 1
        zo_unit = origin(jnp.maximum(unit, 0))

        @pl.when((h == 8) & (z >= Z // 2))
        def _():
            for yo in (y, west, east, across):
                b_wait(lax.rem(z + 4, Z), yo, KEY_COLS, 0)
                b_wait(lax.rem(z + 4, Z), yo, VALUE_COLS, 1)

        @pl.when((unit == 0) | ((unit > 0) & (zo_unit < z)))
        def _():
            a_wait(zo_unit, across, KEY_COLS, 0)
            a_wait(zo_unit, across, VALUE_COLS, 1)

        @pl.when((unit > 0) & (zo_unit < z))
        def _():
            compute(zo_unit, 0, None)

        @pl.when(unit == 0)
        def _():
            compute(z, 0, hidden_keys())

        @pl.when(h == 1)
        def _():
            a_near(lax.rem(z + Z - 1, Z))
            a_near(lax.rem(z + 1, Z))

        def event(j):
            distance = h // 2 + 1
            yo = order(lax.rem(h, 2) * 2 + j // 2)
            ahead, behind = lax.rem(z + Z - distance, Z), lax.rem(z + distance, Z)

            @pl.when((h <= 5) & (j % 2 == 0) & (z >= distance))
            def _():
                b_wait(ahead, yo)

                @pl.when((distance < 3) & (z < Z - 1))
                def _():
                    b_z(ahead, yo, up, 0).start()

                @pl.when((distance == 3) & (z < Z - 1))
                def _():
                    b_z(ahead, yo, up, 0, KEY_COLS, 0).start()

            @pl.when((h <= 5) & (j % 2 == 1) & (behind < Z // 2))
            def _():
                b_wait(behind, yo)

                @pl.when(distance < 3)
                def _():
                    b_z(behind, yo, down, 1).start()

                @pl.when(distance == 3)
                def _():
                    b_z(behind, yo, down, 1, VALUE_COLS, 1).start()

            slot = (h - 1) * 2 + j // 2

            @pl.when((h >= 1) & (j % 2 == 0) & (slot == z))
            def _():
                @pl.when(z > 0)
                def _():
                    chain_copy().wait_recv()

                @pl.when(z < Z - 1)
                def _():
                    pass_on()

        @pl.when(h == 1)
        def _():
            for peer in (east, west, across):
                for part, buffer in enumerate((chip_state, chip_decay)):
                    remote(
                        buffer.at[peer],
                        buffer.at[peer],
                        line_send.at[0, part],
                        line_recv.at[peer, part],
                        sp_1=peer,
                    ).wait_recv()

        for j in range(4):
            event(j)
        return carry

    lax.fori_loop(0, 9, half_step, 0)

    lane = lax.broadcasted_iota(jnp.int32, (chip_rows, 128), 1)
    for group in range(4):
        summed = jnp.sum(total_ref[group], axis=1, keepdims=True)
        stat_ref[group] = jnp.where(lane < 64, top_ref[group], summed)
    theirs = pl.ds(pl.multiple_of(other * tok_rows, tok_rows), tok_rows)
    mine = pl.ds(pl.multiple_of(core * tok_rows, tok_rows), tok_rows)
    swap_numer = remote(
        numer_ref.at[:, theirs], far_numer, pair_send.at[3], pair_recv.at[3], sp_2=other
    )
    swap_stat = remote(
        stat_ref.at[:, theirs], far_stat, pair_send.at[4], pair_recv.at[4], sp_2=other
    )
    swap_numer.start()
    swap_stat.start()

    state = chain_ref[0]
    for yo in range(Y - 1):
        state = jnp.where(yo < y, follow(state, yo), state)
    after = as_column(jnp.exp(core_decay[0][:1])) * state + core_state[0]
    state = jnp.where(core == 1, after, state)
    rows = local_ref[...] + jnp.dot(
        reach_ref[...], state, precision=HIGHEST, preferred_element_type=jnp.float32
    )
    act_ref[:, 2 * VAL_DIM :] = head_norm(rows, lin_gain_ref[...]).astype(act_ref.dtype)

    swap_numer.wait_recv()
    swap_stat.wait_recv()

    def merged(group):
        near, far = stat_ref[group, mine], far_stat[group]
        near_top, far_top = near[:, :1], far[:, :1]
        both_top = jnp.maximum(near_top, far_top)
        near_scale, far_scale = jnp.exp2(near_top - both_top), jnp.exp2(far_top - both_top)
        total = near[:, 64:65] * near_scale + far[:, 64:65] * far_scale
        numer = numer_ref[group, mine] * near_scale + far_numer[group] * far_scale
        return numer / total

    for head in range(2):
        attended = merged(head) - lam_ref[head] * merged(2 + head)
        act_ref[:, head * VAL_DIM : (head + 1) * VAL_DIM] = head_norm(
            attended, diff_gain_ref[...]
        ).astype(act_ref.dtype)

    own_rows = tok_rows // TP
    half = COLUMNS // 2
    halves = (slice(0, half), slice(half, COLUMNS))
    rows_of = lambda member: pl.ds(pl.multiple_of(member * own_rows, own_rows), own_rows)
    toward = (right, left)
    opposite = lax.rem(x + 2, TP)
    for copy in weights:
        copy.wait()

    def far_copy(chunk, way):
        return remote(
            part_ref.at[chunk, rows_of(opposite), halves[way]],
            far_in.at[chunk, way],
            far_send.at[chunk, way],
            far_recv.at[chunk, way],
            tp=toward[way],
        )

    def near_copy(chunk, way):
        return remote(
            near_out.at[chunk, way],
            near_in.at[chunk, way],
            near_send.at[chunk, way],
            near_recv.at[chunk, way],
            tp=toward[way],
        )

    chunks = part_ref.shape[0]

    def project(chunk, carry):
        first = pl.multiple_of(chunk * COLUMNS, COLUMNS)
        part_ref[chunk] = jnp.dot(
            act_ref[...], w_ref[:, pl.ds(first, COLUMNS)], preferred_element_type=jnp.float32
        ).astype(part_ref.dtype)
        for way in range(2):
            far_copy(chunk, way).start()
        return carry

    lax.fori_loop(0, chunks, project, 0)

    def meet(chunk, carry):
        for way in range(2):
            far_copy(chunk, way).wait_recv()
            near = part_ref[chunk, rows_of(toward[way])].astype(jnp.float32)
            here = near[:, halves[way]] + far_in[chunk, way].astype(jnp.float32)
            sides = (here, near[:, halves[1]]) if way == 0 else (near[:, halves[0]], here)
            near_out[chunk, way] = jnp.concatenate(sides, axis=1).astype(near_out.dtype)
            near_copy(chunk, way).start()
        return carry

    lax.fori_loop(0, chunks, meet, 0)

    def finish(chunk, carry):
        total = part_ref[chunk, rows_of(x)].astype(jnp.float32)
        for way in range(2):
            near_copy(chunk, way).wait_recv()
            total = total + near_in[chunk, way].astype(jnp.float32)
        first = pl.multiple_of(chunk * COLUMNS, COLUMNS)
        out_ref[:, pl.ds(first, COLUMNS)] = total.astype(out_ref.dtype)
        return carry

    lax.fori_loop(0, chunks, finish, 0)

    def drain_out(chunk, carry):
        for way in range(2):
            far_copy(chunk, way).wait_send()
            near_copy(chunk, way).wait_send()
        return carry

    lax.fori_loop(0, chunks, drain_out, 0)
    for copy in (pair_q, pair_state, pair_decay, swap_numer, swap_stat):
        copy.wait_send()
    for index, peer in enumerate((east, west, across)):
        for copy in line(peer, index):
            copy.wait_send()

    @pl.when(z < Z - 1)
    def _():
        chain_copy().wait_send()

    for way, toward in ((0, east), (1, west)):
        b_y(toward, way).wait_send()
        b_far(west if way == 0 else east, toward, way).wait_send()

    def drain(offset, carry):
        zo = z - offset
        for way, toward in ((0, east), (1, west)):
            a_y(zo, toward, way).wait_send()
            a_far(zo, west if way == 0 else east, toward, way).wait_send()
        return carry

    lax.fori_loop(0, z + 1, drain, 0)

    @pl.when(z < Z - 1)
    def _():
        def drain_up(offset, carry):
            a_z(z - offset, up, 0).wait_send()
            for yo in range(Y):
                b_z(z - offset, yo, up, 0).wait_send()
            return carry

        lax.fori_loop(0, jnp.minimum(z + 1, 3), drain_up, 0)

        @pl.when(z >= 3)
        def _():
            a_z(z - 3, up, 0, KEY_COLS, 0).wait_send()
            for yo in range(Y):
                b_z(z - 3, yo, up, 0, KEY_COLS, 0).wait_send()

    for distance in range(4):
        zo = lax.rem(z + distance, Z)
        part = (VALUE_COLS, 1) if distance == 3 else ()

        @pl.when(zo < Z // 2)
        def _(zo=zo, part=part):
            a_z(zo, down, 1, *part).wait_send()
            for yo in range(Y):
                b_z(zo, yo, down, 1, *part).wait_send()


def body(
    queries,
    keys,
    values,
    lam,
    diff_gain,
    lin_query,
    lin_key,
    lin_value,
    decay_pre,
    lin_gain,
    w_out_diff,
    w_out_lin,
):
    tok_rows = queries.shape[0]
    depth = w_out_diff.shape[0] + w_out_lin.shape[0]
    model = w_out_diff.shape[1]
    chunks, own_rows = model // COLUMNS, tok_rows // TP
    rows = 2 * tok_rows
    width = 2 * HEAD_DIM + VAL_DIM
    in_hbm = pl.BlockSpec(memory_space=pl.ANY)
    in_vmem = pl.BlockSpec(memory_space=pltpu.VMEM)
    dma = pltpu.SemaphoreType.DMA
    return pl.pallas_call(
        mixer_kernel,
        out_shape=jax.ShapeDtypeStruct((own_rows, model), jnp.bfloat16),
        in_specs=[in_hbm] * 3
        + [pl.BlockSpec(memory_space=pltpu.SMEM)]
        + [in_vmem] * 6
        + [in_hbm] * 2,
        out_specs=in_vmem,
        scratch_shapes=[
            pltpu.VMEM((tok_rows, 3 * VAL_DIM), jnp.bfloat16),
            pltpu.VMEM((depth, model), jnp.bfloat16),
            pltpu.VMEM((chunks, tok_rows, COLUMNS), jnp.bfloat16),
            pltpu.VMEM((chunks, 2, own_rows, COLUMNS // 2), jnp.bfloat16),
            pltpu.VMEM((chunks, 2, own_rows, COLUMNS), jnp.bfloat16),
            pltpu.VMEM((chunks, 2, own_rows, COLUMNS), jnp.bfloat16),
            pltpu.VMEM((Z, Y, FIRST, width), jnp.bfloat16),
            pltpu.VMEM((Z, Y, SECOND, width), jnp.bfloat16),
            pltpu.VMEM((2, tok_rows, 4 * HEAD_DIM), jnp.bfloat16),
            pltpu.VMEM((4, rows, 2 * HEAD_DIM), jnp.bfloat16),
            pltpu.VMEM((4, rows, 128), jnp.float32),
            pltpu.VMEM((4, rows, 128), jnp.float32),
            pltpu.VMEM((4, rows, VAL_DIM), jnp.float32),
            pltpu.VMEM((4, rows, 128), jnp.float32),
            pltpu.VMEM((4, tok_rows, 128), jnp.float32),
            pltpu.VMEM((4, tok_rows, VAL_DIM), jnp.float32),
            pltpu.VMEM((tok_rows, VAL_DIM), jnp.float32),
            pltpu.VMEM((tok_rows, KEY_DIM), jnp.float32),
            pltpu.VMEM((2, KEY_DIM, VAL_DIM), jnp.float32),
            pltpu.VMEM((2, 8, KEY_DIM), jnp.float32),
            pltpu.VMEM((Y, KEY_DIM, VAL_DIM), jnp.bfloat16),
            pltpu.VMEM((Y, 8, KEY_DIM), jnp.float32),
            pltpu.VMEM((2, KEY_DIM, VAL_DIM), jnp.float32),
            dma((5,)),
            dma((Z, Y, 2)),
            dma((Z, Y, 2)),
            dma((Z, 2)),
            dma((Z, 2)),
            dma((Z, 2)),
            dma((2,)),
            dma((2,)),
            dma((Z, Y, 2)),
            dma((5,)),
            dma((5,)),
            dma((3, 2)),
            dma((Y, 2)),
            dma((1,)),
            dma((1,)),
            dma((2,)),
            dma((chunks, 2)),
            dma((chunks, 2)),
            dma((chunks, 2)),
            dma((chunks, 2)),
        ],
        compiler_params=pltpu.CompilerParams(
            collective_id=0, has_side_effects=True, vmem_limit_bytes=60 * 1024 * 1024
        ),
        cost_estimate=pl.CostEstimate(
            flops=12 * 10**9, bytes_accessed=16 * 10**6, transcendentals=16 * 10**6
        ),
    )(
        queries,
        keys,
        values,
        lam,
        diff_gain.reshape(1, VAL_DIM),
        lin_query,
        lin_key,
        lin_value,
        decay_pre,
        lin_gain.reshape(1, VAL_DIM),
        w_out_diff,
        w_out_lin,
    )


def solution(mesh):
    finer = Mesh(mesh.devices.reshape(8, 4, 2, mesh.shape["tp"]), ("sp_0", "sp_1", "sp_2", "tp"))
    in_specs = (
        P(SP, "tp"),
        P(SP, "tp"),
        P(SP, "tp"),
        P("tp"),
        P(),
        P(SP, "tp"),
        P(SP, "tp"),
        P(SP, "tp"),
        P(SP, "tp"),
        P("tp"),
        P("tp", None),
        P("tp", None),
    )
    out_specs = P(SP_TP, None)
    return jax.shard_map(body, mesh=finer, in_specs=in_specs, out_specs=out_specs, check_vma=False)
```
